128 devices in a mesh: fs: 16 (over z, y), tp: 8 (over x, core).
Axes of the slice: x: 4, y: 4, z: 4, core: 2. Of those that a mesh axis runs over, the one named last changes fastest.
Arguments:
- normed_input: bfloat16 [24576, 2048], P(('fs', 'tp')), may hold values from -6 to 6
- pre_act: bfloat16 [24576, 8192], P('fs', 'tp'), may hold values from -6 to 6
- out_grad: bfloat16 [24576, 2048], P(('fs', 'tp')), may hold values from -24 to 24
- up_weight: bfloat16 [2048, 8192], P('fs', 'tp'), may hold values from -0.125 to 0.125
- down_weight: bfloat16 [8192, 2048], P('tp', 'fs'), may hold values from -0.0625 to 0.0625
Outputs:
- input_grad: bfloat16 [24576, 2048], P(('fs', 'tp'))
- up_grad: float32 [2048, 8192], P('fs', 'tp')
- down_grad: float32 [8192, 2048], P('tp', 'fs')
The draws below stay inside these ranges and needn't reach their ends.
All inputs are finite; a program needn't handle non-finite values.
Results may differ from the reference program's by a relative error of at most 0.014.
Values may be sent and summed in bfloat16 or wider, within the bound.
A program may use at most 128 MiB of HBM per device.

```python
import jax
import jax.numpy as jnp
from jax import lax

D = 2048
FF = 8192
TOKENS = 24576
N_TP = 8


def raised(values, stream_key, source, target, blocks, factor):
    owner, partner = [(jnp.arange(values.shape[dim]) // (values.shape[dim] // blocks)).reshape([-1 if axis == dim else 1 for axis in range(values.ndim)]) for dim in (source, target)]
    chosen = jax.random.permutation(stream_key, blocks)[partner]
    strong = (owner == chosen) | (owner == (partner + blocks // 2) % blocks)
    return jnp.where(strong, factor * values, values)


def shard_levels(stream_key, extent, split, smallest, high):
    gain, own = 1.0, jax.random.fold_in(stream_key, 6)
    for position, shards_of in split:
        steps = jnp.exp(jax.random.uniform(jax.random.fold_in(own, position), (shards_of,), jnp.float32, smallest / len(split), high / len(split)))
        gain = gain * jnp.repeat(steps, extent[position] // shards_of).reshape([-1 if axis == position else 1 for axis in range(len(extent))])
    return gain


def centred(key, shape, scale, limit, cuts=(), dtype=jnp.bfloat16):
    drawn = jax.random.normal(key, shape, jnp.float32) * scale
    if len(cuts) > 0:
        drawn = shard_levels(key, shape, cuts, -0.22, 0.18) * drawn
    return jnp.clip(drawn, min=-limit, max=limit).astype(dtype)


def heavy_noise(stream_key, dims, spread, most, cuts, heavy, kind=jnp.bfloat16):
    result = spread * jax.random.normal(stream_key, dims, jnp.float32)
    if cuts:
        result = result * shard_levels(stream_key, dims, cuts, -0.22, 0.18)
    return jnp.clip(raised(result, jax.random.fold_in(stream_key, 3), *heavy), -most, most).astype(kind)


def setup_inputs(seed: int = 0) -> dict:
    streams_of = jax.random.split(jax.random.key(seed), 6)
    normed_input = centred(streams_of[0], (TOKENS, D), 1.0, 6.0, ((0, 128),))
    pre_act = centred(streams_of[1], (TOKENS, FF), 1.0, 6.0, ((0, 16), (1, 8)))
    out_grad = heavy_noise(streams_of[2], (TOKENS, D), 1.0, 24.0, ((0, 128),), (0, 1, 128, 5.5))
    up_weight = centred(streams_of[3], (D, FF), D ** -0.5, 0.125, ((0, 16), (1, 8)))
    down_weight = centred(streams_of[4], (FF, D), FF ** -0.5, 0.0625, ((0, 8), (1, 16)))
    return {"normed_input": normed_input, "pre_act": pre_act, "out_grad": out_grad, "up_weight": up_weight, "down_weight": down_weight}


def reference(normed_input, pre_act, out_grad, up_weight, down_weight):
    active = jnp.maximum(pre_act.astype(jnp.float32), 0.0)
    hidden = (active * active).astype(jnp.bfloat16)
    width = FF // N_TP
    up_blocks = up_weight.reshape(D, N_TP, width).transpose(1, 0, 2)
    down_blocks = down_weight.reshape(N_TP, width, D)
    act_blocks = active.reshape(TOKENS, N_TP, width).transpose(1, 0, 2)
    hid_blocks = hidden.reshape(TOKENS, N_TP, width).transpose(1, 0, 2)

    def one_block(items):
        up_part, down_part, act_part, hid_part = items
        grad_hidden = jnp.dot(out_grad, down_part.T, preferred_element_type=jnp.float32)
        pre_grad = (2.0 * act_part * grad_hidden).astype(jnp.bfloat16)
        part = jnp.dot(pre_grad, up_part.T, preferred_element_type=jnp.float32).astype(jnp.bfloat16)
        up_part_grad = jnp.dot(normed_input.T, pre_grad, preferred_element_type=jnp.float32)
        down_part_grad = jnp.dot(hid_part.T, out_grad, preferred_element_type=jnp.float32)
        return part, up_part_grad, down_part_grad

    parts, up_grads, down_grads = lax.map(one_block, (up_blocks, down_blocks, act_blocks, hid_blocks))
    input_grad = jnp.sum(parts.astype(jnp.float32), axis=0).astype(jnp.bfloat16)
    up_grad = up_grads.transpose(1, 0, 2).reshape(D, FF)
    down_grad = down_grads.reshape(FF, D)
    return input_grad, up_grad, down_grad
```

```python
import jax
import jax.numpy as jnp
from jax import lax
from jax.experimental import pallas as pl
from jax.experimental.pallas import tpu as pltpu
from jax.sharding import PartitionSpec as P

MESH = pl.DeviceIdType.MESH
F32 = jnp.float32
BF16 = jnp.bfloat16
SEMS = 160


def rem4(value):
    return lax.rem(value, 4)


def nt(a, b):
    return lax.dot_general(a, b, (((1,), (1,)), ((), ())), preferred_element_type=F32)


def nn(a, b):
    return jnp.dot(a, b, preferred_element_type=F32)


class Wires:
    def __init__(self, send_sem, recv_sem, partner):
        self.send_sem, self.recv_sem, self.partner = send_sem, recv_sem, partner
        self.numbers, self.sent = {}, []

    def number(self, key):
        return self.numbers.setdefault(key, len(self.numbers))

    def copy(self, k, src, dst, device):
        return pltpu.make_async_remote_copy(
            src_ref=src,
            dst_ref=dst,
            send_sem=self.send_sem.at[k],
            recv_sem=self.recv_sem.at[k],
            device_id=device,
            device_id_type=MESH,
        )

    def send(self, key, src, dst, device):
        k = self.number(key)
        self.copy(k, src(), dst(), device).start()
        self.sent.append((key, src))

    def recv(self, key, ref):
        self.copy(self.number(key), ref(), ref(), self.partner).wait_recv()

    def drain(self, tag=None):
        for key, src in self.sent:
            if tag is None or key[0] == tag:
                k = self.number(key)
                self.copy(k, src(), src(), self.partner).wait_send()
        self.sent = [s for s in self.sent if not (tag is None or s[0][0] == tag)]


class Gather:
    def __init__(self, wires, tag, pos, right, left, piece):
        self.w, self.tag, self.pos = wires, tag, pos
        self.right, self.left, self.piece = right, left, piece

    def at(self, hop, p):
        return lambda: self.piece(rem4(self.pos + hop), p)

    def put(self, name, hop, p, device):
        self.w.send((self.tag, name), self.at(hop, p), self.at(hop, p), device)

    def got(self, name, hop, p):
        self.w.recv((self.tag, name), self.at(hop, p))

    def own(self):
        self.put("R0", 0, 0, self.right)
        self.put("L0", 0, 1, self.left)
        self.put("R1", 0, 1, self.right)
        self.put("L1", 0, 0, self.left)

    def forward(self):
        self.got("R0", 3, 0)
        self.put("R2", 3, 0, self.right)
        self.got("L0", 1, 1)
        self.put("L2", 1, 1, self.left)

    def near(self):
        self.got("R1", 3, 1)
        self.got("L1", 1, 0)

    def far(self):
        self.got("R2", 2, 0)
        self.got("L2", 2, 1)


class Scatter:
    def __init__(self, wires, tag, pos, right, left, piece, landing):
        self.w, self.tag, self.pos = wires, tag, pos
        self.right, self.left = right, left
        self.piece, self.landing = piece, landing

    def at(self, hop, p):
        return lambda: self.piece(rem4(self.pos + hop), p)

    def put(self, side, m, hop, p):
        self.w.send(
            (self.tag, side, m),
            self.at(hop, p),
            lambda: self.landing(side, m),
            self.right if side == 0 else self.left,
        )

    def got(self, side, m):
        self.w.recv((self.tag, side, m), lambda: self.landing(side, m))
        return self.landing(side, m)

    def far(self):
        self.put(0, 0, 2, 0)
        self.put(1, 0, 2, 1)

    def to_right(self):
        self.put(0, 1, 1, 1)

    def to_left(self):
        self.put(1, 1, 3, 0)

    def middle(self):
        for side, hop, p in ((0, 1, 0), (1, 3, 1)):
            came = self.got(side, 0)
            mine = self.at(hop, p)()
            mine[...] = (mine[...].astype(F32) + came[...].astype(F32)).astype(BF16)
            self.put(side, 2, hop, p)

    def finish(self, out=None):
        for p, a, b in ((1, (0, 1), (1, 2)), (0, (1, 1), (0, 2))):
            first, second = self.got(*a), self.got(*b)
            mine = self.at(0, p)()
            total = mine[...].astype(F32) + first[...].astype(F32) + second[...].astype(F32)
            target = mine if out is None else out(p)
            target[...] = total.astype(target.dtype)


def kernel(
    ni_hbm, pa_hbm, og_hbm, uw_hbm, dw_hbm,
    ig_hbm, ug_hbm, dg_hbm,
    ni, og, wd, wu, pg, ht, pgt, part, gd, gu,
    cross, xland, zland_d, yland_d, yone_d, zone_d,
    zland_u, yland_u, yone_u, zone_u,
    dg, ug, send_sem, recv_sem, local_sem,
):
    fs, tp = lax.axis_index("fs"), lax.axis_index("tp")
    z, y, x, c = fs // 4, rem4(fs), tp // 2, lax.rem(tp, 2)
    x_right = {"fs": fs, "tp": rem4(x + 1) * 2 + c}
    x_left = {"fs": fs, "tp": rem4(x + 3) * 2 + c}
    y_right = {"fs": z * 4 + rem4(y + 1), "tp": tp}
    y_left = {"fs": z * 4 + rem4(y + 3), "tp": tp}
    z_right = {"fs": rem4(z + 1) * 4 + y, "tp": tp}
    z_left = {"fs": rem4(z + 3) * 4 + y, "tp": tp}
    partner = {"fs": fs, "tp": x * 2 + 1 - c}

    rows = og_hbm.shape[0]
    half = rows // 2
    ff, cols = dw_hbm.shape
    wide = 4 * cols
    quarter = ff // 4
    urows = uw_hbm.shape[0]
    tokens = pg.shape[0]

    w = Wires(send_sem, recv_sem, partner)

    def token_rows(ref, block):
        return ref.at[pl.ds(pl.multiple_of(block * rows, rows), rows), :]

    def lanes(i):
        return pl.ds(pl.multiple_of(i * cols, cols), cols)

    mine = [
        (dw_hbm, wd.at[z, :, lanes(y)]),
        (og_hbm, token_rows(og, tp)),
        (uw_hbm, wu.at[z, y]),
        (pa_hbm, pg),
        (ni_hbm, token_rows(ni, tp)),
    ]
    local = [
        pltpu.make_async_copy(src, dst, local_sem.at[i])
        for i, (src, dst) in enumerate(mine)
    ]
    for copy in local:
        copy.start()

    barrier = pltpu.get_barrier_semaphore()
    for device in (x_right, x_left, y_right, y_left, z_right, z_left, partner):
        pl.semaphore_signal(barrier, inc=1, device_id=device, device_id_type=MESH)
    pl.semaphore_wait(barrier, 7)

    def wd_rows(p):
        return pl.ds(p * quarter, quarter)

    def wu_rows(p):
        return pl.ds(p * (urows // 4), urows // 4)

    def weight_rings(tag, one, z_group, y_group):
        return (
            (
                Gather(w, tag + "a1", y, y_right, y_left, lambda i, p: one(z, i, p)),
                Gather(w, tag + "b1", z, z_right, z_left, lambda i, p: one(i, y, 2 + p)),
            ),
            (
                Gather(w, tag + "a2", z, z_right, z_left, lambda i, p: z_group(i, p)),
                Gather(w, tag + "b2", y, y_right, y_left, lambda i, p: y_group(i, 2 + p)),
            ),
        )

    wd1, wd2 = weight_rings(
        "d",
        lambda zi, yi, p: wd.at[zi, wd_rows(p), lanes(yi)],
        lambda zi, p: wd.at[zi, wd_rows(p), :],
        lambda yi, p: wd.at[:, wd_rows(p), lanes(yi)],
    )
    wu1, wu2 = weight_rings(
        "u",
        lambda zi, yi, p: wu.at[zi, yi, wu_rows(p), :],
        lambda zi, p: wu.at[zi, :, wu_rows(p), :],
        lambda yi, p: wu.at[:, yi, wu_rows(p), :],
    )

    def token_piece(ref, core):
        def piece(i, p):
            start = pl.multiple_of((i * 2 + core) * rows + p * half, half)
            return ref.at[pl.ds(start, half), :]

        return piece

    rings = {
        "o": Gather(w, "o", x, x_right, x_left, token_piece(og, c)),
        "n": Gather(w, "n", x, x_right, x_left, token_piece(ni, c)),
    }
    others = {"o": token_piece(og, 1 - c), "n": token_piece(ni, 1 - c)}

    def hand(tag, *pieces):
        for hop, p in pieces:
            ref = rings[tag].at(hop, p)
            w.send((tag, "c", hop, p), ref, ref, partner)

    def handed(tag):
        for hop in range(4):
            for p in range(2):
                w.recv((tag, "c", hop, p), lambda: others[tag](rem4(x + hop), p))

    def token_own(tag):
        rings[tag].own()
        hand(tag, (0, 0), (0, 1))

    def token_forward(tag):
        rings[tag].forward()
        hand(tag, (3, 0), (1, 1))

    def token_near(tag):
        rings[tag].near()
        hand(tag, (3, 1), (1, 0))

    def token_far(tag):
        rings[tag].far()
        hand(tag, (2, 0), (2, 1))

    def each(pair, step):
        for ring in pair:
            getattr(ring, step)()

    def hidden(count, first):
        def body(j, carry):
            at = pl.multiple_of(j * 128, 128)
            active = jnp.maximum(pg[pl.ds(at, 128), :].astype(F32), 0.0)
            ht[:, pl.ds(at, 128)] = (active * active).astype(BF16).T
            return carry

        lax.fori_loop(first, first + count, body, 0)

    local[0].wait()
    each(wd1, "own")
    local[1].wait()
    token_own("o")
    local[3].wait()
    hidden(3, 0)
    each(wd1, "forward")
    local[2].wait()
    each(wu1, "own")
    hidden(3, 3)
    each(wd1, "near")
    each(wd1, "far")
    each(wu1, "forward")
    each(wd2, "own")
    hidden(3, 6)
    token_forward("o")
    local[4].wait()
    token_own("n")
    each(wu1, "near")
    each(wu1, "far")
    hidden(3, 9)
    each(wd2, "forward")
    each(wu2, "own")
    token_near("o")
    each(wd2, "near")
    each(wd2, "far")
    token_far("o")
    handed("o")

    block = 256

    def pre_grad(i, carry):
        at = pl.ds(pl.multiple_of(i * block, block), block)
        weight = jnp.concatenate([wd[k] for k in range(4)], axis=1)
        grad = nt(og[at, :], weight)
        active = jnp.maximum(pg[at, :].astype(F32), 0.0)
        value = (2.0 * active * grad).astype(BF16)
        pg[at, :] = value
        pgt[:, at] = value.T

        @pl.when(i == 2)
        def _():
            each(wu2, "forward")

        @pl.when(i == 4)
        def _():
            token_forward("n")

        return carry

    lax.fori_loop(0, tokens // block, pre_grad, 0)

    def grad_rings(tag, grad, zland, yland, yone, zone):
        return (
            (
                Scatter(
                    w, tag + "a1", z, z_right, z_left,
                    lambda i, p: grad.at[i, wd_rows(p), :],
                    lambda side, m: zland.at[side, m],
                ),
                Scatter(
                    w, tag + "b1", y, y_right, y_left,
                    lambda i, p: grad.at[:, wd_rows(2 + p), lanes(i)],
                    lambda side, m: yland.at[side, m],
                ),
            ),
            (
                Scatter(
                    w, tag + "a2", y, y_right, y_left,
                    lambda i, p: grad.at[z, wd_rows(p), lanes(i)],
                    lambda side, m: yone.at[side, m],
                ),
                Scatter(
                    w, tag + "b2", z, z_right, z_left,
                    lambda i, p: grad.at[i, wd_rows(2 + p), lanes(y)],
                    lambda side, m: zone.at[side, m],
                ),
            ),
        )

    gd1, gd2 = grad_rings("D", gd, zland_d, yland_d, yone_d, zone_d)
    gu1, gu2 = grad_rings("U", gu, zland_u, yland_u, yone_u, zone_u)
    upper = ff // 2

    def hop_of(k):
        return jnp.where(k == 0, 2, jnp.where(k == 1, 1, jnp.where(k == 2, 3, 0)))

    def weight_grad(left, right, grad, first, extra):
        def body(k, carry):
            zi, yi = rem4(z + hop_of(k)), rem4(y + hop_of(k))
            strip = right[:, pl.ds(pl.multiple_of(zi * wide, wide), wide)]
            grad[zi, :upper, :] = nn(left[:upper, :], strip).astype(BF16)
            strip = jnp.concatenate(
                [right[:, pl.ds(pl.multiple_of(g * wide + yi * cols, cols), cols)] for g in range(4)],
                axis=1,
            )
            value = nn(left[upper:, :], strip).astype(BF16)
            for g in range(4):
                grad[g, upper:, lanes(yi)] = value[:, g * cols : (g + 1) * cols]

            for turn, step in ((0, "far"), (1, "to_right"), (2, "to_left")):

                @pl.when(k == turn)
                def _(step=step):
                    each(first, step)

            extra(k)
            return carry

        lax.fori_loop(0, 4, body, 0)

    def while_down(k):
        @pl.when(k == 2)
        def _():
            token_near("n")

    weight_grad(ht, og, gd, gd1, while_down)

    each(wu2, "near")
    each(wu2, "far")

    def share(block):
        return part.at[block]

    xs = Scatter(
        w, "x", x, x_right, x_left,
        lambda i, p: part.at[i * 2 + c, pl.ds(p * half, half), :],
        lambda side, m: xland.at[side, m],
    )
    cross_base = w.number(("cross", 0))
    for k in range(1, 4):
        w.number(("cross", k))

    def product(index):
        at = pl.ds(pl.multiple_of(index * rows, rows), rows)
        weight = wu[...].reshape(16 * urows, ff)
        part[index] = nt(pg[at, :], weight).astype(BF16)

    def add_cross(k):
        index = rem4(x + hop_of(k)) * 2 + c
        w.copy(cross_base + k, cross.at[k], cross.at[k], partner).wait_recv()
        total = part[index].astype(F32) + cross[k].astype(F32)
        part[index] = total.astype(BF16)

    def input_grad(k, carry):
        xi = rem4(x + hop_of(k))
        product(xi * 2 + 1 - c)
        w.copy(cross_base + k, part.at[xi * 2 + 1 - c], cross.at[k], partner).start()

        @pl.when(k > 0)
        def _():
            add_cross(k - 1)

        for turn, step in ((1, xs.far), (2, xs.to_right), (3, xs.to_left)):

            @pl.when(k == turn)
            def _(step=step):
                step()

        product(xi * 2 + c)

        @pl.when(k == 1)
        def _():
            token_far("n")

        @pl.when(k == 2)
        def _():
            each(gd1, "middle")

        return carry

    lax.fori_loop(0, 4, input_grad, 0)
    add_cross(3)
    handed("n")

    def while_up(k):
        @pl.when(k == 2)
        def _():
            xs.middle()

        @pl.when(k == 3)
        def _():
            each(gd1, "finish")
            each(gd2, "far")
            each(gd2, "to_right")
            each(gd2, "to_left")

    weight_grad(pgt, ni, gu, gu1, while_up)

    each(gu1, "middle")
    each(gd2, "middle")

    def own_rows(out):
        return (
            lambda p: out.at[wd_rows(p), :],
            lambda p: out.at[wd_rows(2 + p), :],
        )

    for ring, out in zip(gd2, own_rows(dg)):
        ring.finish(out)
    down_out = pltpu.make_async_copy(dg, dg_hbm, local_sem.at[5])
    down_out.start()
    w.drain("o")
    ig = og.at[pl.ds(0, rows), :]
    xs.finish(lambda p: og.at[pl.ds(p * half, half), :])
    input_out = pltpu.make_async_copy(ig, ig_hbm, local_sem.at[6])
    input_out.start()
    each(gu1, "finish")
    each(gu2, "far")
    each(gu2, "to_right")
    each(gu2, "to_left")
    each(gu2, "middle")
    for ring, out in zip(gu2, own_rows(ug)):
        ring.finish(out)
    up_out = pltpu.make_async_copy(ug, ug_hbm, local_sem.at[7])
    up_out.start()
    for k in range(4):
        w.copy(cross_base + k, cross.at[k], cross.at[k], partner).wait_send()
    w.drain()
    down_out.wait()
    input_out.wait()
    up_out.wait()


def local(normed_input, pre_act, out_grad, up_weight, down_weight):
    rows, d = out_grad.shape
    tokens, ff = pre_act.shape
    cols = down_weight.shape[1]
    quarter = ff // 4
    half = rows // 2
    grads = [
        pltpu.VMEM((2, 3, quarter, 4 * cols), BF16),
        pltpu.VMEM((2, 3, 4, quarter, cols), BF16),
        pltpu.VMEM((2, 3, quarter, cols), BF16),
        pltpu.VMEM((2, 3, quarter, cols), BF16),
    ]
    input_grad, up_grad, down_grad = pl.pallas_call(
        kernel,
        out_shape=(
            jax.ShapeDtypeStruct((rows, d), BF16),
            jax.ShapeDtypeStruct((ff, cols), F32),
            jax.ShapeDtypeStruct((ff, cols), F32),
        ),
        in_specs=[pl.BlockSpec(memory_space=pl.ANY)] * 5,
        out_specs=(pl.BlockSpec(memory_space=pl.ANY),) * 3,
        scratch_shapes=[
            pltpu.VMEM((tokens, d), BF16),
            pltpu.VMEM((tokens, d), BF16),
            pltpu.VMEM((4, ff, 4 * cols), BF16),
            pltpu.VMEM((4, 4, d // 16, ff), BF16),
            pltpu.VMEM((tokens, ff), BF16),
            pltpu.VMEM((ff, tokens), BF16),
            pltpu.VMEM((ff, tokens), BF16),
            pltpu.VMEM((8, rows, d), BF16),
            pltpu.VMEM((4, ff, 4 * cols), BF16),
            pltpu.VMEM((4, ff, 4 * cols), BF16),
            pltpu.VMEM((4, rows, d), BF16),
            pltpu.VMEM((2, 3, half, d), BF16),
            *grads,
            *grads,
            pltpu.VMEM((ff, cols), F32),
            pltpu.VMEM((ff, cols), F32),
            pltpu.SemaphoreType.DMA((SEMS,)),
            pltpu.SemaphoreType.DMA((SEMS,)),
            pltpu.SemaphoreType.DMA((8,)),
        ],
        compiler_params=pltpu.CompilerParams(
            collective_id=0,
            has_side_effects=True,
            vmem_limit_bytes=67043328,
        ),
        name="ffn_backward",
    )(normed_input, pre_act, out_grad, up_weight, down_weight)
    return input_grad, up_grad.T, down_grad


def solution(mesh):
    placed = (
        P(("fs", "tp"), None),
        P("fs", "tp"),
        P(("fs", "tp"), None),
        P("fs", "tp"),
        P("tp", "fs"),
    )
    return jax.shard_map(
        local,
        mesh=mesh,
        in_specs=placed,
        out_specs=(P(("fs", "tp"), None), P("fs", "tp"), P("tp", "fs")),
        check_vma=False,
    )
```

```python
import math

import jax
import jax.numpy as jnp
from jax import lax
from jax.experimental import pallas as pl
from jax.experimental.pallas import tpu as pltpu
from jax.sharding import PartitionSpec as P

MESH = pl.DeviceIdType.MESH
F32 = jnp.float32
BF16 = jnp.bfloat16
SENDS, RECVS = 8, 64


def rem4(value):
    return lax.rem(value, 4)


def nt(a, b):
    return lax.dot_general(a, b, (((1,), (1,)), ((), ())), preferred_element_type=F32)


def nn(a, b):
    return jnp.dot(a, b, preferred_element_type=F32)


def size_of(ref):
    return 2 * math.prod(ref.shape)


class Wires:
    def __init__(self, send_sem, recv_sem, partner, filler):
        self.send_sem, self.recv_sem, self.partner = send_sem, recv_sem, partner
        self.filler = filler
        self.groups, self.keys, self.bytes = {}, {}, {}

    def group(self, name):
        return self.groups.setdefault(name, len(self.groups))

    def key(self, name):
        return self.keys.setdefault(name, len(self.keys))

    def copy(self, g, k, src, dst, device):
        return pltpu.make_async_remote_copy(
            src_ref=src,
            dst_ref=dst,
            send_sem=self.send_sem.at[g],
            recv_sem=self.recv_sem.at[k],
            device_id=device,
            device_id_type=MESH,
        )

    def send(self, group, key, src, dst, device):
        self.copy(self.group(group), self.key(key), src, dst, device).start()
        self.bytes[group] = self.bytes.get(group, 0) + size_of(src)

    def recv(self, key, size):
        ref = self.filler(size)
        self.copy(0, self.key(key), ref, ref, self.partner).wait_recv()

    def drain(self, group):
        ref = self.filler(self.bytes[group])
        self.copy(self.group(group), 0, ref, ref, self.partner).wait_send()


class Gather:
    def __init__(self, wires, group, tag, pos, right, left, piece):
        self.w, self.group, self.tag, self.pos = wires, group, tag, pos
        self.right, self.left, self.piece = right, left, piece
        self.size = size_of(piece(pos, 0))

    def at(self, hop, p):
        return self.piece(rem4(self.pos + hop), p)

    def put(self, name, hop, p, device):
        ref = self.at(hop, p)
        self.w.send(self.group, (self.tag, name), ref, ref, device)

    def own(self):
        self.put("first", 0, 0, self.right)
        self.put("first", 0, 1, self.left)
        self.put("near", 0, 1, self.right)
        self.put("near", 0, 0, self.left)

    def forward(self):
        self.w.recv((self.tag, "first"), 2 * self.size)
        self.put("far", 3, 0, self.right)
        self.put("far", 1, 1, self.left)

    def near(self):
        self.w.recv((self.tag, "near"), 2 * self.size)

    def far(self):
        self.w.recv((self.tag, "far"), 2 * self.size)


class QuarterGather(Gather):
    def __init__(self, wires, group, tag, pos, right, left, piece, quarter):
        super().__init__(wires, group, tag, pos, right, left, piece)
        self.quarter = quarter

    def give(self, turn, *members):
        name = (self.tag, "near" if turn else "first")
        for h in members:
            for device, p in ((self.right, turn), (self.left, 1 - turn)):
                ref = self.quarter(self.pos, p, h)
                self.w.send(self.group, name, ref, ref, device)


class Scatter:
    def __init__(self, wires, group, tag, pos, right, left, piece, landing):
        self.w, self.group, self.tag, self.pos = wires, group, tag, pos
        self.right, self.left = right, left
        self.piece, self.landing = piece, landing
        self.size = size_of(piece(pos, 0))

    def at(self, hop, p):
        return self.piece(rem4(self.pos + hop), p)

    def put(self, name, side, m, hop, p):
        self.w.send(
            self.group,
            (self.tag, name),
            self.at(hop, p),
            self.landing(side, m),
            self.right if side == 0 else self.left,
        )

    def far(self):
        self.put("first", 0, 0, 2, 0)
        self.put("first", 1, 0, 2, 1)

    def to_right(self):
        self.put("last", 0, 1, 1, 1)

    def to_left(self):
        self.put("last", 1, 1, 3, 0)

    def add_first(self):
        self.w.recv((self.tag, "first"), 2 * self.size)
        for side, hop, p in ((0, 1, 0), (1, 3, 1)):
            came, mine = self.landing(side, 0), self.at(hop, p)
            mine[...] = (mine[...].astype(F32) + came[...].astype(F32)).astype(BF16)

    def middle(self):
        self.add_first()
        self.put("last", 0, 2, 1, 0)
        self.put("last", 1, 2, 3, 1)

    def finish(self, out=None):
        self.w.recv((self.tag, "last"), 4 * self.size)
        for p, near, far in ((1, 0, 1), (0, 1, 0)):
            first, second = self.landing(near, 1), self.landing(far, 2)
            mine = self.at(0, p)
            total = mine[...].astype(F32) + first[...].astype(F32) + second[...].astype(F32)
            target = mine if out is None else out(p)
            target[...] = total.astype(target.dtype)


class QuarterScatter(Scatter):
    def __init__(self, wires, group, tag, pos, right, left, piece, landing, quarter, landed):
        super().__init__(wires, group, tag, pos, right, left, piece, landing)
        self.quarter, self.landed = quarter, landed

    def give(self, *members):
        for h in members:
            for side, hop, p in ((0, 1, 0), (1, 3, 1)):
                self.w.send(
                    self.group,
                    (self.tag, h),
                    self.quarter(rem4(self.pos + hop), p, h),
                    self.landed(side, 2, h),
                    self.right if side == 0 else self.left,
                )

    def settle_near(self):
        self.w.recv((self.tag, "last"), 2 * self.size)

    def settle(self, h):
        self.w.recv((self.tag, h), self.size // 2)
        for p, near, far in ((1, 0, 1), (0, 1, 0)):
            first, second = self.landed(near, 1, h), self.landed(far, 2, h)
            mine = self.quarter(self.pos, p, h)
            total = mine[...].astype(F32) + first[...].astype(F32) + second[...].astype(F32)
            mine[...] = total.astype(BF16)


def kernel(
    ni_hbm, pa_hbm, og_hbm, uw_hbm, dw_hbm,
    ig_hbm, ug_hbm, dg_hbm,
    ni, og, wd, wu, pg, ht, pgt, part, gd, gu,
    cross, xland, zland_d, yland_d, yone_d, zone_d,
    zland_u, yland_u, yone_u, zone_u,
    dg, ug, send_sem, recv_sem, local_sem,
):
    fs, tp = lax.axis_index("fs"), lax.axis_index("tp")
    z, y, x, c = fs // 4, rem4(fs), tp // 2, lax.rem(tp, 2)
    x_right = {"fs": fs, "tp": rem4(x + 1) * 2 + c}
    x_left = {"fs": fs, "tp": rem4(x + 3) * 2 + c}
    y_right = {"fs": z * 4 + rem4(y + 1), "tp": tp}
    y_left = {"fs": z * 4 + rem4(y + 3), "tp": tp}
    z_right = {"fs": rem4(z + 1) * 4 + y, "tp": tp}
    z_left = {"fs": rem4(z + 3) * 4 + y, "tp": tp}
    partner = {"fs": fs, "tp": x * 2 + 1 - c}

    rows = og_hbm.shape[0]
    half = rows // 2
    ff, cols = dw_hbm.shape
    wide = 4 * cols
    quarter = ff // 4
    urows = uw_hbm.shape[0]
    tokens = pg.shape[0]

    line = 2 * og.shape[1]
    w = Wires(send_sem, recv_sem, partner, lambda size: og.at[pl.ds(0, size // line), :])

    def token_rows(ref, block):
        return ref.at[pl.ds(pl.multiple_of(block * rows, rows), rows), :]

    def lanes(i):
        return pl.ds(pl.multiple_of(i * cols, cols), cols)

    mine = [
        (dw_hbm, wd.at[z, :, lanes(y)]),
        (og_hbm, token_rows(og, tp)),
        (uw_hbm, wu.at[z, y]),
        (pa_hbm, pg),
        (ni_hbm, token_rows(ni, tp)),
    ]
    local = [
        pltpu.make_async_copy(src, dst, local_sem.at[i])
        for i, (src, dst) in enumerate(mine)
    ]
    for copy in local:
        copy.start()

    barrier = pltpu.get_barrier_semaphore()
    for device in (x_right, x_left, y_right, y_left, z_right, z_left, partner):
        pl.semaphore_signal(barrier, inc=1, device_id=device, device_id_type=MESH)
    pl.semaphore_wait(barrier, 7)

    def wd_rows(p):
        return pl.ds(p * quarter, quarter)

    def wu_rows(p):
        return pl.ds(p * (urows // 4), urows // 4)

    def weight_rings(tag, one, z_group, y_group):
        return (
            (
                Gather(w, tag, tag + "a1", y, y_right, y_left, lambda i, p: one(z, i, p)),
                Gather(w, tag, tag + "b1", z, z_right, z_left, lambda i, p: one(i, y, 2 + p)),
            ),
            (
                Gather(w, tag, tag + "a2", z, z_right, z_left, lambda i, p: z_group(i, p)),
                Gather(w, tag, tag + "b2", y, y_right, y_left, lambda i, p: y_group(i, 2 + p)),
            ),
        )

    wd1, _ = weight_rings(
        "d",
        lambda zi, yi, p: wd.at[zi, wd_rows(p), lanes(yi)],
        lambda zi, p: wd.at[zi, wd_rows(p), :],
        lambda yi, p: wd.at[:, wd_rows(p), lanes(yi)],
    )
    wd2 = (
        QuarterGather(
            w, "d", "da2", z, z_right, z_left,
            lambda i, p: wd.at[i, wd_rows(p), :],
            lambda i, p, h: wd.at[i, wd_rows(p), lanes(rem4(y + h))],
        ),
        QuarterGather(
            w, "d", "db2", y, y_right, y_left,
            lambda i, p: wd.at[:, wd_rows(2 + p), lanes(i)],
            lambda i, p, h: wd.at[rem4(z + h), wd_rows(2 + p), lanes(i)],
        ),
    )
    wu1, wu2 = weight_rings(
        "u",
        lambda zi, yi, p: wu.at[zi, yi, wu_rows(p), :],
        lambda zi, p: wu.at[zi, :, wu_rows(p), :],
        lambda yi, p: wu.at[:, yi, wu_rows(p), :],
    )

    def token_piece(ref, core):
        def piece(i, p):
            start = pl.multiple_of((i * 2 + core) * rows + p * half, half)
            return ref.at[pl.ds(start, half), :]

        return piece

    rings = {
        "o": Gather(w, "o", "o", x, x_right, x_left, token_piece(og, c)),
        "n": Gather(w, "n", "n", x, x_right, x_left, token_piece(ni, c)),
    }

    def hand(tag, *pieces):
        for hop, p in pieces:
            ref = rings[tag].at(hop, p)
            w.send(tag, (tag, "cross"), ref, ref, partner)

    def handed(tag):
        w.recv((tag, "cross"), 8 * rings[tag].size)

    def token_own(tag):
        rings[tag].own()
        hand(tag, (0, 0), (0, 1))

    def token_forward(tag):
        rings[tag].forward()
        hand(tag, (3, 0), (1, 1))

    def token_near(tag):
        rings[tag].near()
        hand(tag, (3, 1), (1, 0))

    def token_far(tag):
        rings[tag].far()
        hand(tag, (2, 0), (2, 1))

    def each(pair, step):
        for ring in pair:
            getattr(ring, step)()

    def hidden(count, first):
        def body(j, carry):
            at = pl.multiple_of(j * 128, 128)
            active = jnp.maximum(pg[pl.ds(at, 128), :].astype(F32), 0.0)
            ht[:, pl.ds(at, 128)] = (active * active).astype(BF16).T
            return carry

        lax.fori_loop(first, first + count, body, 0)

    def give(pair, *what):
        for ring in pair:
            ring.give(*what)

    local[0].wait()
    each(wd1, "own")
    local[1].wait()
    token_own("o")
    local[2].wait()
    each(wu1, "own")
    give(wd2, 0, 0)
    give(wd2, 1, 0)
    local[3].wait()
    hidden(6, 0)
    each(wd1, "forward")
    each(wu1, "forward")
    hidden(6, 6)
    each(wd1, "near")
    give(wd2, 0, 1, 3)
    token_forward("o")
    each(wd1, "far")
    give(wd2, 0, 2)
    give(wd2, 1, 1, 3, 2)
    local[4].wait()
    token_own("n")
    each(wu1, "near")
    each(wu1, "far")
    each(wd2, "forward")
    each(wu2, "own")
    token_near("o")
    each(wd2, "near")
    each(wd2, "far")
    token_far("o")
    handed("o")

    block = 256

    def pre_grad(i, carry):
        at = pl.ds(pl.multiple_of(i * block, block), block)
        weight = jnp.concatenate([wd[k] for k in range(4)], axis=1)
        grad = nt(og[at, :], weight)
        active = jnp.maximum(pg[at, :].astype(F32), 0.0)
        value = (2.0 * active * grad).astype(BF16)
        pg[at, :] = value
        pgt[:, at] = value.T

        @pl.when(i == 3)
        def _():
            each(wu2, "forward")

        @pl.when(i == 5)
        def _():
            token_forward("n")

        return carry

    lax.fori_loop(0, tokens // block, pre_grad, 0)

    def grad_rings(tag, grad, zland, yland, yone, zone):
        return (
            (
                Scatter(
                    w, tag, tag + "a1", z, z_right, z_left,
                    lambda i, p: grad.at[i, wd_rows(p), :],
                    lambda side, m: zland.at[side, m],
                ),
                Scatter(
                    w, tag, tag + "b1", y, y_right, y_left,
                    lambda i, p: grad.at[:, wd_rows(2 + p), lanes(i)],
                    lambda side, m: yland.at[side, m],
                ),
            ),
            (
                Scatter(
                    w, tag, tag + "a2", y, y_right, y_left,
                    lambda i, p: grad.at[z, wd_rows(p), lanes(i)],
                    lambda side, m: yone.at[side, m],
                ),
                Scatter(
                    w, tag, tag + "b2", z, z_right, z_left,
                    lambda i, p: grad.at[i, wd_rows(2 + p), lanes(y)],
                    lambda side, m: zone.at[side, m],
                ),
            ),
        )

    gd1, gd2 = grad_rings("D", gd, zland_d, yland_d, yone_d, zone_d)
    _, gu2 = grad_rings("U", gu, zland_u, yland_u, yone_u, zone_u)
    gu1 = (
        QuarterScatter(
            w, "U", "Ua1", z, z_right, z_left,
            lambda i, p: gu.at[i, wd_rows(p), :],
            lambda side, m: zland_u.at[side, m],
            lambda i, p, h: gu.at[i, wd_rows(p), lanes(rem4(y + h))],
            lambda side, m, h: zland_u.at[side, m, :, lanes(rem4(y + h))],
        ),
        QuarterScatter(
            w, "U", "Ub1", y, y_right, y_left,
            lambda i, p: gu.at[:, wd_rows(2 + p), lanes(i)],
            lambda side, m: yland_u.at[side, m],
            lambda i, p, h: gu.at[rem4(z + h), wd_rows(2 + p), lanes(i)],
            lambda side, m, h: yland_u.at[side, m, rem4(z + h)],
        ),
    )
    upper = ff // 2

    def hop_of(k):
        return jnp.where(k == 0, 2, jnp.where(k == 1, 1, jnp.where(k == 2, 3, 0)))

    def weight_grad(left, right, grad, first, extra):
        def body(k, carry):
            zi, yi = rem4(z + hop_of(k)), rem4(y + hop_of(k))
            strip = right[:, pl.ds(pl.multiple_of(zi * wide, wide), wide)]
            grad[zi, :upper, :] = nn(left[:upper, :], strip).astype(BF16)
            strip = jnp.concatenate(
                [right[:, pl.ds(pl.multiple_of(g * wide + yi * cols, cols), cols)] for g in range(4)],
                axis=1,
            )
            value = nn(left[upper:, :], strip).astype(BF16)
            for g in range(4):
                grad[g, upper:, lanes(yi)] = value[:, g * cols : (g + 1) * cols]

            if extra:
                extra(k)
            for turn, step in ((0, "far"), (1, "to_right"), (2, "to_left")):

                @pl.when(k == turn)
                def _(step=step):
                    each(first, step)

            return carry

        lax.fori_loop(0, 4, body, 0)

    weight_grad(ht, og, gd, gd1, None)

    each(wu2, "near")
    each(wu2, "far")

    def share(block):
        return part.at[block]

    xs = Scatter(
        w, "x", "x", x, x_right, x_left,
        lambda i, p: part.at[i * 2 + c, pl.ds(p * half, half), :],
        lambda side, m: xland.at[side, m],
    )
    cross_base = [w.key(("c", k)) for k in range(4)][0]
    cross_group = w.group("c")
    w.bytes["c"] = size_of(cross)

    def product(index):
        at = pl.ds(pl.multiple_of(index * rows, rows), rows)
        weight = wu[...].reshape(16 * urows, ff)
        part[index] = nt(pg[at, :], weight).astype(BF16)

    def add_cross(k):
        index = rem4(x + hop_of(k)) * 2 + c
        w.copy(cross_group, cross_base + k, cross.at[k], cross.at[k], partner).wait_recv()
        total = part[index].astype(F32) + cross[k].astype(F32)
        part[index] = total.astype(BF16)

    def input_grad(k, carry):
        xi = rem4(x + hop_of(k))
        product(xi * 2 + 1 - c)
        w.copy(cross_group, cross_base + k, part.at[xi * 2 + 1 - c], cross.at[k], partner).start()

        @pl.when(k > 0)
        def _():
            add_cross(k - 1)

        for turn, step in ((1, xs.far), (2, xs.to_right), (3, xs.to_left)):

            @pl.when(k == turn)
            def _(step=step):
                step()

        product(xi * 2 + c)

        @pl.when(k == 0)
        def _():
            token_near("n")

        @pl.when(k == 1)
        def _():
            each(gd1, "middle")

        @pl.when(k == 2)
        def _():
            token_far("n")

        return carry

    lax.fori_loop(0, 4, input_grad, 0)
    add_cross(3)
    handed("n")

    def while_up(k):
        @pl.when(k == 1)
        def _():
            each(gd1, "finish")
            each(gd2, "far")
            each(gd2, "to_right")
            each(gd2, "to_left")

        @pl.when(k == 2)
        def _():
            xs.middle()

    weight_grad(pgt, ni, gu, gu1, while_up)

    each(gu1, "add_first")
    give(gu1, 2, 1, 3)
    each(gd2, "middle")

    def own_rows(out):
        return (
            lambda p: out.at[wd_rows(p), :],
            lambda p: out.at[wd_rows(2 + p), :],
        )

    def settle(h):
        for ring in gu1:
            ring.settle(h)

    each(gu1, "settle_near")
    settle(2)
    each(gu2, "far")
    give(gu1, 0)
    settle(1)
    each(gu2, "to_right")
    settle(3)
    each(gu2, "to_left")
    w.drain("o")
    ig = og.at[pl.ds(0, rows), :]
    xs.finish(lambda p: og.at[pl.ds(p * half, half), :])
    input_out = pltpu.make_async_copy(ig, ig_hbm, local_sem.at[6])
    input_out.start()
    for ring, out in zip(gd2, own_rows(dg)):
        ring.finish(out)
    down_out = pltpu.make_async_copy(dg, dg_hbm, local_sem.at[5])
    down_out.start()
    each(gu2, "middle")
    settle(0)
    for ring, out in zip(gu2, own_rows(ug)):
        ring.finish(out)
    up_out = pltpu.make_async_copy(ug, ug_hbm, local_sem.at[7])
    up_out.start()
    for group in ("d", "u", "n", "D", "U", "x", "c"):
        w.drain(group)
    down_out.wait()
    input_out.wait()
    up_out.wait()


def deliver(ig_in, ug_in, dg_in, ig_out, ug_out, dg_out, ig, ug, dg, turned, sem):
    into = [
        pltpu.make_async_copy(src, dst, sem.at[i])
        for i, (src, dst) in enumerate(((ug_in, ug), (ig_in, ig), (dg_in, dg)))
    ]
    for copy in into:
        copy.start()
    out = [
        pltpu.make_async_copy(src, dst, sem.at[3 + i])
        for i, (src, dst) in enumerate(((turned, ug_out), (ig, ig_out), (dg, dg_out)))
    ]
    into[0].wait()
    turned[...] = ug[...].T
    out[0].start()
    for i in (1, 2):
        into[i].wait()
        out[i].start()
    for copy in out:
        copy.wait()


def local(normed_input, pre_act, out_grad, up_weight, down_weight):
    rows, d = out_grad.shape
    tokens, ff = pre_act.shape
    cols = down_weight.shape[1]
    quarter = ff // 4
    half = rows // 2
    grads = [
        pltpu.VMEM((2, 3, quarter, 4 * cols), BF16),
        pltpu.VMEM((2, 3, 4, quarter, cols), BF16),
        pltpu.VMEM((2, 3, quarter, cols), BF16),
        pltpu.VMEM((2, 3, quarter, cols), BF16),
    ]
    input_grad, up_grad, down_grad = pl.pallas_call(
        kernel,
        out_shape=(
            jax.ShapeDtypeStruct((rows, d), BF16),
            jax.ShapeDtypeStruct((ff, cols), F32),
            jax.ShapeDtypeStruct((ff, cols), F32),
        ),
        in_specs=[pl.BlockSpec(memory_space=pl.ANY)] * 5,
        out_specs=(pl.BlockSpec(memory_space=pl.ANY),) * 3,
        scratch_shapes=[
            pltpu.VMEM((tokens, d), BF16),
            pltpu.VMEM((tokens, d), BF16),
            pltpu.VMEM((4, ff, 4 * cols), BF16),
            pltpu.VMEM((4, 4, d // 16, ff), BF16),
            pltpu.VMEM((tokens, ff), BF16),
            pltpu.VMEM((ff, tokens), BF16),
            pltpu.VMEM((ff, tokens), BF16),
            pltpu.VMEM((8, rows, d), BF16),
            pltpu.VMEM((4, ff, 4 * cols), BF16),
            pltpu.VMEM((4, ff, 4 * cols), BF16),
            pltpu.VMEM((4, rows, d), BF16),
            pltpu.VMEM((2, 3, half, d), BF16),
            *grads,
            *grads,
            pltpu.VMEM((ff, cols), F32),
            pltpu.VMEM((ff, cols), F32),
            pltpu.SemaphoreType.DMA((SENDS,)),
            pltpu.SemaphoreType.DMA((RECVS,)),
            pltpu.SemaphoreType.DMA((8,)),
        ],
        compiler_params=pltpu.CompilerParams(
            collective_id=0,
            has_side_effects=True,
            vmem_limit_bytes=67043328,
        ),
        name="ffn_backward",
    )(normed_input, pre_act, out_grad, up_weight, down_weight)
    return pl.pallas_call(
        deliver,
        out_shape=(
            jax.ShapeDtypeStruct((rows, d), BF16),
            jax.ShapeDtypeStruct((cols, ff), F32),
            jax.ShapeDtypeStruct((ff, cols), F32),
        ),
        in_specs=[pl.BlockSpec(memory_space=pl.ANY)] * 3,
        out_specs=(pl.BlockSpec(memory_space=pl.ANY),) * 3,
        scratch_shapes=[
            pltpu.VMEM((rows, d), BF16),
            pltpu.VMEM((ff, cols), F32),
            pltpu.VMEM((ff, cols), F32),
            pltpu.VMEM((cols, ff), F32),
            pltpu.SemaphoreType.DMA((6,)),
        ],
        compiler_params=pltpu.CompilerParams(vmem_limit_bytes=67043328),
        name="deliver",
    )(input_grad, up_grad, down_grad)


def solution(mesh):
    placed = (
        P(("fs", "tp"), None),
        P("fs", "tp"),
        P(("fs", "tp"), None),
        P("fs", "tp"),
        P("tp", "fs"),
    )
    return jax.shard_map(
        local,
        mesh=mesh,
        in_specs=placed,
        out_specs=(P(("fs", "tp"), None), P("fs", "tp"), P("tp", "fs")),
        check_vma=False,
    )
```

```python
import math

import jax
import jax.numpy as jnp
from jax import lax
from jax.experimental import pallas as pl
from jax.experimental.pallas import tpu as pltpu
from jax.sharding import PartitionSpec as P

MESH = pl.DeviceIdType.MESH
F32 = jnp.float32
BF16 = jnp.bfloat16
SENDS, RECVS = 8, 64


def rem4(value):
    return lax.rem(value, 4)


def nt(a, b):
    return lax.dot_general(a, b, (((1,), (1,)), ((), ())), preferred_element_type=F32)


def nn(a, b):
    return jnp.dot(a, b, preferred_element_type=F32)


def size_of(ref):
    return 2 * math.prod(ref.shape)


class Wires:
    def __init__(self, send_sem, recv_sem, partner, filler):
        self.send_sem, self.recv_sem, self.partner = send_sem, recv_sem, partner
        self.filler = filler
        self.groups, self.keys, self.bytes = {}, {}, {}

    def group(self, name):
        return self.groups.setdefault(name, len(self.groups))

    def key(self, name):
        return self.keys.setdefault(name, len(self.keys))

    def copy(self, g, k, src, dst, device):
        return pltpu.make_async_remote_copy(
            src_ref=src,
            dst_ref=dst,
            send_sem=self.send_sem.at[g],
            recv_sem=self.recv_sem.at[k],
            device_id=device,
            device_id_type=MESH,
        )

    def send(self, group, key, src, dst, device):
        self.copy(self.group(group), self.key(key), src, dst, device).start()
        self.bytes[group] = self.bytes.get(group, 0) + size_of(src)

    def recv(self, key, size):
        ref = self.filler(size)
        self.copy(0, self.key(key), ref, ref, self.partner).wait_recv()

    def drain(self, group):
        ref = self.filler(self.bytes[group])
        self.copy(self.group(group), 0, ref, ref, self.partner).wait_send()


class Gather:
    def __init__(self, wires, group, tag, pos, right, left, piece):
        self.w, self.group, self.tag, self.pos = wires, group, tag, pos
        self.right, self.left, self.piece = right, left, piece
        self.size = size_of(piece(pos, 0))

    def at(self, hop, p):
        return self.piece(rem4(self.pos + hop), p)

    def put(self, name, hop, p, device):
        ref = self.at(hop, p)
        self.w.send(self.group, (self.tag, name), ref, ref, device)

    def own(self):
        self.put("first", 0, 0, self.right)
        self.put("first", 0, 1, self.left)
        self.put("near", 0, 1, self.right)
        self.put("near", 0, 0, self.left)

    def forward(self):
        self.w.recv((self.tag, "first"), 2 * self.size)
        self.put("far", 3, 0, self.right)
        self.put("far", 1, 1, self.left)

    def near(self):
        self.w.recv((self.tag, "near"), 2 * self.size)

    def far(self):
        self.w.recv((self.tag, "far"), 2 * self.size)


class QuarterGather(Gather):
    def __init__(self, wires, group, tag, pos, right, left, piece, quarter):
        super().__init__(wires, group, tag, pos, right, left, piece)
        self.quarter = quarter

    def give(self, turn, *members):
        name = (self.tag, "near" if turn else "first")
        for h in members:
            for device, p in ((self.right, turn), (self.left, 1 - turn)):
                ref = self.quarter(self.pos, p, h)
                self.w.send(self.group, name, ref, ref, device)


class Scatter:
    def __init__(self, wires, group, tag, pos, right, left, piece, landing):
        self.w, self.group, self.tag, self.pos = wires, group, tag, pos
        self.right, self.left = right, left
        self.piece, self.landing = piece, landing
        self.size = size_of(piece(pos, 0))

    def at(self, hop, p):
        return self.piece(rem4(self.pos + hop), p)

    def put(self, name, side, m, hop, p):
        self.w.send(
            self.group,
            (self.tag, name),
            self.at(hop, p),
            self.landing(side, m),
            self.right if side == 0 else self.left,
        )

    def far(self):
        self.put("first", 0, 0, 2, 0)
        self.put("first", 1, 0, 2, 1)

    def to_right(self):
        self.put("last", 0, 1, 1, 1)

    def to_left(self):
        self.put("last", 1, 1, 3, 0)

    def add_first(self):
        self.w.recv((self.tag, "first"), 2 * self.size)
        for side, hop, p in ((0, 1, 0), (1, 3, 1)):
            came, mine = self.landing(side, 0), self.at(hop, p)
            mine[...] = (mine[...].astype(F32) + came[...].astype(F32)).astype(BF16)

    def middle(self):
        self.add_first()
        self.put("last", 0, 2, 1, 0)
        self.put("last", 1, 2, 3, 1)

    def finish(self, store=None):
        self.w.recv((self.tag, "last"), 4 * self.size)
        for p, near, far in ((1, 0, 1), (0, 1, 0)):
            first, second = self.landing(near, 1), self.landing(far, 2)
            mine = self.at(0, p)
            total = mine[...].astype(F32) + first[...].astype(F32) + second[...].astype(F32)
            if store is None:
                mine[...] = total.astype(BF16)
            else:
                store(p, total)


class QuarterScatter(Scatter):
    def __init__(self, wires, group, tag, pos, right, left, piece, landing, quarter, landed):
        super().__init__(wires, group, tag, pos, right, left, piece, landing)
        self.quarter, self.landed = quarter, landed

    def give(self, *members):
        for h in members:
            for side, hop, p in ((0, 1, 0), (1, 3, 1)):
                self.w.send(
                    self.group,
                    (self.tag, h),
                    self.quarter(rem4(self.pos + hop), p, h),
                    self.landed(side, 2, h),
                    self.right if side == 0 else self.left,
                )

    def settle_near(self):
        self.w.recv((self.tag, "last"), 2 * self.size)

    def settle(self, h):
        self.w.recv((self.tag, h), self.size // 2)
        for p, near, far in ((1, 0, 1), (0, 1, 0)):
            first, second = self.landed(near, 1, h), self.landed(far, 2, h)
            mine = self.quarter(self.pos, p, h)
            total = mine[...].astype(F32) + first[...].astype(F32) + second[...].astype(F32)
            mine[...] = total.astype(BF16)


def kernel(
    ni_hbm, pa_hbm, og_hbm, uw_hbm, dw_hbm,
    ig, ug, dg,
    ni, og, wd, wu, pg, ht, pgt, part, gd,
    cross, xland, zland_d, yland_d, yone_d, zone_d,
    zland_u, yland_u, yone_u, zone_u,
    send_sem, recv_sem, local_sem,
):
    fs, tp = lax.axis_index("fs"), lax.axis_index("tp")
    z, y, x, c = fs // 4, rem4(fs), tp // 2, lax.rem(tp, 2)
    x_right = {"fs": fs, "tp": rem4(x + 1) * 2 + c}
    x_left = {"fs": fs, "tp": rem4(x + 3) * 2 + c}
    y_right = {"fs": z * 4 + rem4(y + 1), "tp": tp}
    y_left = {"fs": z * 4 + rem4(y + 3), "tp": tp}
    z_right = {"fs": rem4(z + 1) * 4 + y, "tp": tp}
    z_left = {"fs": rem4(z + 3) * 4 + y, "tp": tp}
    partner = {"fs": fs, "tp": x * 2 + 1 - c}

    rows = og_hbm.shape[0]
    half = rows // 2
    ff, cols = dw_hbm.shape
    wide = 4 * cols
    quarter = ff // 4
    urows = uw_hbm.shape[0]
    tokens = pg.shape[0]

    line = 2 * og.shape[1]
    w = Wires(send_sem, recv_sem, partner, lambda size: og.at[pl.ds(0, size // line), :])

    def token_rows(ref, block):
        return ref.at[pl.ds(pl.multiple_of(block * rows, rows), rows), :]

    def lanes(i):
        return pl.ds(pl.multiple_of(i * cols, cols), cols)

    mine = [
        (dw_hbm, wd.at[z, :, lanes(y)]),
        (og_hbm, token_rows(og, tp)),
        (uw_hbm, wu.at[z, y]),
        (pa_hbm, pg),
        (ni_hbm, token_rows(ni, tp)),
    ]
    local = [
        pltpu.make_async_copy(src, dst, local_sem.at[i])
        for i, (src, dst) in enumerate(mine)
    ]
    barrier = pltpu.get_barrier_semaphore()
    for device in (x_right, x_left, y_right, y_left, z_right, z_left, partner):
        pl.semaphore_signal(barrier, inc=1, device_id=device, device_id_type=MESH)
    for copy in local:
        copy.start()
    pl.semaphore_wait(barrier, 7)

    def wd_rows(p):
        return pl.ds(p * quarter, quarter)

    def wu_rows(p):
        return pl.ds(p * (urows // 4), urows // 4)

    def weight_rings(tag, one, z_group, y_group):
        return (
            (
                Gather(w, tag, tag + "a1", y, y_right, y_left, lambda i, p: one(z, i, p)),
                Gather(w, tag, tag + "b1", z, z_right, z_left, lambda i, p: one(i, y, 2 + p)),
            ),
            (
                Gather(w, tag, tag + "a2", z, z_right, z_left, lambda i, p: z_group(i, p)),
                Gather(w, tag, tag + "b2", y, y_right, y_left, lambda i, p: y_group(i, 2 + p)),
            ),
        )

    wd1, _ = weight_rings(
        "d",
        lambda zi, yi, p: wd.at[zi, wd_rows(p), lanes(yi)],
        lambda zi, p: wd.at[zi, wd_rows(p), :],
        lambda yi, p: wd.at[:, wd_rows(p), lanes(yi)],
    )
    wd2 = (
        QuarterGather(
            w, "d", "da2", z, z_right, z_left,
            lambda i, p: wd.at[i, wd_rows(p), :],
            lambda i, p, h: wd.at[i, wd_rows(p), lanes(rem4(y + h))],
        ),
        QuarterGather(
            w, "d", "db2", y, y_right, y_left,
            lambda i, p: wd.at[:, wd_rows(2 + p), lanes(i)],
            lambda i, p, h: wd.at[rem4(z + h), wd_rows(2 + p), lanes(i)],
        ),
    )
    wu1, wu2 = weight_rings(
        "u",
        lambda zi, yi, p: wu.at[zi, yi, wu_rows(p), :],
        lambda zi, p: wu.at[zi, :, wu_rows(p), :],
        lambda yi, p: wu.at[:, yi, wu_rows(p), :],
    )

    def token_piece(ref, core):
        def piece(i, p):
            start = pl.multiple_of((i * 2 + core) * rows + p * half, half)
            return ref.at[pl.ds(start, half), :]

        return piece

    rings = {
        "o": Gather(w, "o", "o", x, x_right, x_left, token_piece(og, c)),
        "n": Gather(w, "n", "n", x, x_right, x_left, token_piece(ni, c)),
    }

    def hand(tag, *pieces):
        for hop, p in pieces:
            ref = rings[tag].at(hop, p)
            w.send(tag, (tag, "cross"), ref, ref, partner)

    def handed(tag):
        w.recv((tag, "cross"), 8 * rings[tag].size)

    def token_own(tag):
        rings[tag].own()
        hand(tag, (0, 0), (0, 1))

    def token_forward(tag):
        rings[tag].forward()
        hand(tag, (3, 0), (1, 1))

    def token_near(tag):
        rings[tag].near()
        hand(tag, (3, 1), (1, 0))

    def token_far(tag):
        rings[tag].far()
        hand(tag, (2, 0), (2, 1))

    def each(pair, step):
        for ring in pair:
            getattr(ring, step)()

    def hidden(count, first):
        def body(j, carry):
            at = pl.multiple_of(j * 128, 128)
            active = jnp.maximum(pg[pl.ds(at, 128), :].astype(F32), 0.0)
            ht[:, pl.ds(at, 128)] = (active * active).astype(BF16).T
            return carry

        lax.fori_loop(first, first + count, body, 0)

    def give(pair, *what):
        for ring in pair:
            ring.give(*what)

    local[0].wait()
    each(wd1, "own")
    local[1].wait()
    token_own("o")
    local[2].wait()
    each(wu1, "own")
    give(wd2, 0, 0)
    give(wd2, 1, 0)
    local[3].wait()
    hidden(6, 0)
    each(wd1, "forward")
    each(wu1, "forward")
    hidden(6, 6)
    each(wd1, "near")
    give(wd2, 0, 1, 3)
    token_forward("o")
    each(wd1, "far")
    give(wd2, 0, 2)
    give(wd2, 1, 1, 3, 2)
    local[4].wait()
    token_own("n")
    each(wu1, "near")
    each(wu1, "far")
    each(wd2, "forward")
    each(wu2, "own")
    token_near("o")
    each(wd2, "near")
    each(wd2, "far")
    token_far("o")
    handed("o")

    block = 256

    def pre_grad(i, carry):
        at = pl.ds(pl.multiple_of(i * block, block), block)
        for n in range(2):
            units = pl.ds(n * ff // 2, ff // 2)
            weight = jnp.concatenate([wd[k, units, :] for k in range(4)], axis=1)
            grad = nt(og[at, :], weight)
            active = jnp.maximum(pg[at, units].astype(F32), 0.0)
            value = (2.0 * active * grad).astype(BF16)
            pg[at, units] = value
            pgt[units, at] = value.T

        @pl.when(i == 3)
        def _():
            each(wu2, "forward")

        @pl.when(i == 5)
        def _():
            token_forward("n")

        return carry

    lax.fori_loop(0, tokens // block, pre_grad, 0)

    def grad_rings(tag, grad, zland, yland, yone, zone):
        return (
            (
                Scatter(
                    w, tag, tag + "a1", z, z_right, z_left,
                    lambda i, p: grad.at[i, wd_rows(p), :],
                    lambda side, m: zland.at[side, m],
                ),
                Scatter(
                    w, tag, tag + "b1", y, y_right, y_left,
                    lambda i, p: grad.at[:, wd_rows(2 + p), lanes(i)],
                    lambda side, m: yland.at[side, m],
                ),
            ),
            (
                Scatter(
                    w, tag, tag + "a2", y, y_right, y_left,
                    lambda i, p: grad.at[z, wd_rows(p), lanes(i)],
                    lambda side, m: yone.at[side, m],
                ),
                Scatter(
                    w, tag, tag + "b2", z, z_right, z_left,
                    lambda i, p: grad.at[i, wd_rows(2 + p), lanes(y)],
                    lambda side, m: zone.at[side, m],
                ),
            ),
        )

    gd1, gd2 = grad_rings("D", gd, zland_d, yland_d, yone_d, zone_d)
    gu = wd
    _, gu2 = grad_rings("U", gu, zland_u, yland_u, yone_u, zone_u)
    gu1 = (
        QuarterScatter(
            w, "U", "Ua1", z, z_right, z_left,
            lambda i, p: gu.at[i, wd_rows(p), :],
            lambda side, m: zland_u.at[side, m],
            lambda i, p, h: gu.at[i, wd_rows(p), lanes(rem4(y + h))],
            lambda side, m, h: zland_u.at[side, m, :, lanes(rem4(y + h))],
        ),
        QuarterScatter(
            w, "U", "Ub1", y, y_right, y_left,
            lambda i, p: gu.at[:, wd_rows(2 + p), lanes(i)],
            lambda side, m: yland_u.at[side, m],
            lambda i, p, h: gu.at[rem4(z + h), wd_rows(2 + p), lanes(i)],
            lambda side, m, h: yland_u.at[side, m, rem4(z + h)],
        ),
    )
    upper = ff // 2

    def hop_of(k):
        return jnp.where(k == 0, 2, jnp.where(k == 1, 1, jnp.where(k == 2, 3, 0)))

    def weight_grad(left, right, grad, first, extra):
        def body(k, carry):
            zi, yi = rem4(z + hop_of(k)), rem4(y + hop_of(k))
            strip = right[:, pl.ds(pl.multiple_of(zi * wide, wide), wide)]
            grad[zi, :upper, :] = nn(left[:upper, :], strip).astype(BF16)
            strip = jnp.concatenate(
                [right[:, pl.ds(pl.multiple_of(g * wide + yi * cols, cols), cols)] for g in range(4)],
                axis=1,
            )
            value = nn(left[upper:, :], strip).astype(BF16)
            for g in range(4):
                grad[g, upper:, lanes(yi)] = value[:, g * cols : (g + 1) * cols]

            if extra:
                extra(k)
            for turn, step in ((0, "far"), (1, "to_right"), (2, "to_left")):

                @pl.when(k == turn)
                def _(step=step):
                    each(first, step)

            return carry

        lax.fori_loop(0, 4, body, 0)

    weight_grad(ht, og, gd, gd1, None)

    each(wu2, "near")
    each(wu2, "far")

    def share(block):
        return part.at[block]

    xs = Scatter(
        w, "x", "x", x, x_right, x_left,
        lambda i, p: part.at[i * 2 + c, pl.ds(p * half, half), :],
        lambda side, m: xland.at[side, m],
    )
    cross_base = [w.key(("c", k)) for k in range(4)][0]
    cross_group = w.group("c")
    w.bytes["c"] = size_of(cross)

    def product(xi):
        at = pl.ds(pl.multiple_of(xi * 2 * rows, 2 * rows), 2 * rows)
        for g in range(4):
            value = nt(pg[at, :], wu[g].reshape(4 * urows, ff)).astype(BF16)
            out = pl.ds(g * 4 * urows, 4 * urows)
            part[xi * 2, :, out] = value[:rows]
            part[xi * 2 + 1, :, out] = value[rows:]

    def send_cross(k):
        block = part.at[rem4(x + hop_of(k)) * 2 + 1 - c]
        w.copy(cross_group, cross_base + k, block, cross.at[k], partner).start()

    def add_cross(k):
        index = rem4(x + hop_of(k)) * 2 + c
        w.copy(cross_group, cross_base + k, cross.at[k], cross.at[k], partner).wait_recv()
        total = part[index].astype(F32) + cross[k].astype(F32)
        part[index] = total.astype(BF16)

    def input_grad(k, carry):
        xi = rem4(x + hop_of(k))
        product(xi)
        send_cross(k)

        @pl.when(k > 0)
        def _():
            add_cross(k - 1)

        for turn, step in ((1, xs.far), (2, xs.to_right)):

            @pl.when(k == turn)
            def _(step=step):
                step()

        @pl.when(k == 0)
        def _():
            token_near("n")

        @pl.when(k == 1)
        def _():
            each(gd1, "middle")

        @pl.when(k == 2)
        def _():
            token_far("n")

        return carry

    lax.fori_loop(0, 3, input_grad, 0)
    add_cross(2)
    xs.to_left()
    handed("n")
    w.drain("d")

    def while_up(k):
        @pl.when(k == 1)
        def _():
            each(gd1, "finish")
            each(gd2, "far")
            each(gd2, "to_right")
            each(gd2, "to_left")

        @pl.when(k == 2)
        def _():
            xs.middle()

    weight_grad(pgt, ni, gu, gu1, while_up)

    product(x)
    send_cross(3)
    each(gu1, "add_first")
    give(gu1, 2, 1, 3)
    each(gd2, "middle")
    add_cross(3)

    def settle(h):
        for ring in gu1:
            ring.settle(h)

    each(gu1, "settle_near")
    settle(2)
    each(gu2, "far")
    give(gu1, 0)
    settle(1)
    each(gu2, "to_right")
    settle(3)
    each(gu2, "to_left")

    def store_rows(p, total):
        ig[pl.ds(p * half, half), :] = total.astype(BF16)

    xs.finish(store_rows)
    for i, ring in enumerate(gd2):

        def store_down(p, total, i=i):
            dg[wd_rows(2 * i + p), :] = total

        ring.finish(store_down)
    each(gu2, "middle")
    settle(0)
    for i, ring in enumerate(gu2):

        def store_up(p, total, i=i):
            ug[:, wd_rows(2 * i + p)] = total.T

        ring.finish(store_up)
    for group in ("u", "o", "n", "D", "U", "x", "c"):
        w.drain(group)


def deliver(*refs):
    sem = refs[-1]
    copies = [pltpu.make_async_copy(refs[i], refs[3 + i], sem.at[i]) for i in range(3)]
    for copy in copies:
        copy.start()
    for copy in copies:
        copy.wait()


def local(normed_input, pre_act, out_grad, up_weight, down_weight):
    rows, d = out_grad.shape
    tokens, ff = pre_act.shape
    cols = down_weight.shape[1]
    quarter = ff // 4
    half = rows // 2
    grads = [
        pltpu.VMEM((2, 3, quarter, 4 * cols), BF16),
        pltpu.VMEM((2, 3, 4, quarter, cols), BF16),
        pltpu.VMEM((2, 3, quarter, cols), BF16),
        pltpu.VMEM((2, 3, quarter, cols), BF16),
    ]
    input_grad, up_grad, down_grad = pl.pallas_call(
        kernel,
        out_shape=(
            pltpu.VMEM((rows, d), BF16),
            pltpu.VMEM((cols, ff), F32),
            pltpu.VMEM((ff, cols), F32),
        ),
        in_specs=[pl.BlockSpec(memory_space=pltpu.HBM)] * 5,
        out_specs=(pl.BlockSpec(memory_space=pltpu.VMEM),) * 3,
        scratch_shapes=[
            pltpu.VMEM((tokens, d), BF16),
            pltpu.VMEM((tokens, d), BF16),
            pltpu.VMEM((4, ff, 4 * cols), BF16),
            pltpu.VMEM((4, 4, d // 16, ff), BF16),
            pltpu.VMEM((tokens, ff), BF16),
            pltpu.VMEM((ff, tokens), BF16),
            pltpu.VMEM((ff, tokens), BF16),
            pltpu.VMEM((8, rows, d), BF16),
            pltpu.VMEM((4, ff, 4 * cols), BF16),
            pltpu.VMEM((4, rows, d), BF16),
            pltpu.VMEM((2, 3, half, d), BF16),
            *grads,
            *grads,
            pltpu.SemaphoreType.DMA((SENDS,)),
            pltpu.SemaphoreType.DMA((RECVS,)),
            pltpu.SemaphoreType.DMA((5,)),
        ],
        compiler_params=pltpu.CompilerParams(
            collective_id=0,
            has_side_effects=True,
            vmem_limit_bytes=62800000,
        ),
        name="ffn_backward",
    )(normed_input, pre_act, out_grad, up_weight, down_weight)
    return pl.pallas_call(
        deliver,
        out_shape=(
            jax.ShapeDtypeStruct((rows, d), BF16),
            jax.ShapeDtypeStruct((cols, ff), F32),
            jax.ShapeDtypeStruct((ff, cols), F32),
        ),
        in_specs=[pl.BlockSpec(memory_space=pl.ANY)] * 3,
        out_specs=(pl.BlockSpec(memory_space=pl.ANY),) * 3,
        scratch_shapes=[pltpu.SemaphoreType.DMA((3,))],
        compiler_params=pltpu.CompilerParams(vmem_limit_bytes=4 * 2**20),
        name="deliver",
    )(input_grad, up_grad, down_grad)


def solution(mesh):
    placed = (
        P(("fs", "tp"), None),
        P("fs", "tp"),
        P(("fs", "tp"), None),
        P("fs", "tp"),
        P("tp", "fs"),
    )
    return jax.shard_map(
        local,
        mesh=mesh,
        in_specs=placed,
        out_specs=(P(("fs", "tp"), None), P("fs", "tp"), P("tp", "fs")),
        check_vma=False,
    )
```

```python
import math

import jax
import jax.numpy as jnp
from jax import lax
from jax.experimental import pallas as pl
from jax.experimental.pallas import tpu as pltpu
from jax.sharding import PartitionSpec as P

MESH = pl.DeviceIdType.MESH
F32 = jnp.float32
BF16 = jnp.bfloat16
SENDS, RECVS = 8, 38


def rem4(value):
    return lax.rem(value, 4)


def nt(a, b):
    return lax.dot_general(a, b, (((1,), (1,)), ((), ())), preferred_element_type=F32)


def nn(a, b):
    return jnp.dot(a, b, preferred_element_type=F32)


def size_of(ref):
    return 2 * math.prod(ref.shape)


class Wires:
    def __init__(self, send_sem, recv_sem, partner, filler):
        self.send_sem, self.recv_sem, self.partner = send_sem, recv_sem, partner
        self.filler = filler
        self.groups, self.keys, self.bytes = {}, {}, {}

    def group(self, name):
        return self.groups.setdefault(name, len(self.groups))

    def key(self, name):
        return self.keys.setdefault(name, len(self.keys))

    def copy(self, g, k, src, dst, device):
        return pltpu.make_async_remote_copy(
            src_ref=src,
            dst_ref=dst,
            send_sem=self.send_sem.at[g],
            recv_sem=self.recv_sem.at[k],
            device_id=device,
            device_id_type=MESH,
        )

    def send(self, group, key, src, dst, device):
        self.copy(self.group(group), self.key(key), src, dst, device).start()
        self.bytes[group] = self.bytes.get(group, 0) + size_of(src)

    def recv(self, key, size):
        ref = self.filler(size)
        self.copy(0, self.key(key), ref, ref, self.partner).wait_recv()

    def drain(self, group):
        ref = self.filler(self.bytes[group])
        self.copy(self.group(group), 0, ref, ref, self.partner).wait_send()


class Gather:
    share = 1

    def __init__(self, wires, group, tag, pos, right, left, piece):
        self.w, self.group, self.tag, self.pos = wires, group, tag, pos
        self.right, self.left, self.piece = right, left, piece
        self.size = size_of(piece(pos, 0))

    def wait(self, name, pieces):
        if self.share:
            self.w.recv((self.tag, name), self.share * pieces * self.size)

    def at(self, hop, p):
        return self.piece(rem4(self.pos + hop), p)

    def put(self, name, hop, p, device):
        ref = self.at(hop, p)
        self.w.send(self.group, (self.tag, name), ref, ref, device)

    def own(self):
        self.put("first", 0, 0, self.right)
        self.put("first", 0, 1, self.left)
        self.put("near", 0, 1, self.right)
        self.put("near", 0, 0, self.left)

    def forward(self):
        self.wait("first", 2)
        self.put("far", 3, 0, self.right)
        self.put("far", 1, 1, self.left)

    def near(self):
        self.wait("near", 2)

    def far(self):
        self.wait("far", 2)


class QuarterGather(Gather):
    def __init__(self, wires, group, tag, pos, right, left, piece, quarter):
        super().__init__(wires, group, tag, pos, right, left, piece)
        self.quarter = quarter

    def give(self, turn, *members):
        name = (self.tag, "near" if turn else "first")
        for h in members:
            for device, p in ((self.right, turn), (self.left, 1 - turn)):
                ref = self.quarter(self.pos, p, h)
                self.w.send(self.group, name, ref, ref, device)


class Scatter:
    share = 1

    def __init__(self, wires, group, tag, pos, right, left, piece, landing):
        self.w, self.group, self.tag, self.pos = wires, group, tag, pos
        self.right, self.left = right, left
        self.piece, self.landing = piece, landing
        self.size = size_of(piece(pos, 0))

    def wait(self, name, quarters):
        if self.share:
            self.w.recv((self.tag, name), self.share * quarters * self.size // 4)

    def at(self, hop, p):
        return self.piece(rem4(self.pos + hop), p)

    def put(self, name, side, m, hop, p):
        self.w.send(
            self.group,
            (self.tag, name),
            self.at(hop, p),
            self.landing(side, m),
            self.right if side == 0 else self.left,
        )

    def far(self):
        self.put("first", 0, 0, 2, 0)
        self.put("first", 1, 0, 2, 1)

    def to_right(self):
        self.put("last", 0, 1, 1, 1)

    def to_left(self):
        self.put("last", 1, 1, 3, 0)

    def add_first(self):
        self.wait("first", 8)
        for side, hop, p in ((0, 1, 0), (1, 3, 1)):
            came, mine = self.landing(side, 0), self.at(hop, p)
            mine[...] = (mine[...].astype(F32) + came[...].astype(F32)).astype(BF16)

    def middle(self):
        self.add_first()
        self.put("last", 0, 2, 1, 0)
        self.put("last", 1, 2, 3, 1)

    def finish(self, store=None):
        self.wait("last", 16)
        for p, near, far in ((1, 0, 1), (0, 1, 0)):
            first, second = self.landing(near, 1), self.landing(far, 2)
            mine = self.at(0, p)
            total = mine[...].astype(F32) + first[...].astype(F32) + second[...].astype(F32)
            if store is None:
                mine[...] = total.astype(BF16)
            else:
                store(p, total)


class QuarterScatter(Scatter):
    def __init__(self, wires, group, tag, pos, right, left, piece, landing, quarter, landed):
        super().__init__(wires, group, tag, pos, right, left, piece, landing)
        self.quarter, self.landed = quarter, landed

    def give(self, *members):
        for h in members:
            for side, hop, p in ((0, 1, 0), (1, 3, 1)):
                self.w.send(
                    self.group,
                    (self.tag, h),
                    self.quarter(rem4(self.pos + hop), p, h),
                    self.landed(side, 2, h),
                    self.right if side == 0 else self.left,
                )

    def settle_near(self):
        self.wait("last", 8)

    def settle(self, h):
        self.wait(h, 2)
        for p, near, far in ((1, 0, 1), (0, 1, 0)):
            first, second = self.landed(near, 1, h), self.landed(far, 2, h)
            mine = self.quarter(self.pos, p, h)
            total = mine[...].astype(F32) + first[...].astype(F32) + second[...].astype(F32)
            mine[...] = total.astype(BF16)


def paired(first, second):
    second.tag, first.share, second.share = first.tag, 2, 0
    return first, second


def kernel(
    ni_hbm, pa_hbm, og_hbm, uw_hbm, dw_hbm,
    ig, ug, dg,
    ni, og, wd, wu, pg, ht, pgt, part, gd,
    cross, xland, zland_d, yland_d, yone_d, zone_d,
    zland_u, yland_u, yone_u, zone_u,
    send_sem, recv_sem, local_sem,
):
    fs, tp = lax.axis_index("fs"), lax.axis_index("tp")
    z, y, x, c = fs // 4, rem4(fs), tp // 2, lax.rem(tp, 2)
    x_right = {"fs": fs, "tp": rem4(x + 1) * 2 + c}
    x_left = {"fs": fs, "tp": rem4(x + 3) * 2 + c}
    y_right = {"fs": z * 4 + rem4(y + 1), "tp": tp}
    y_left = {"fs": z * 4 + rem4(y + 3), "tp": tp}
    z_right = {"fs": rem4(z + 1) * 4 + y, "tp": tp}
    z_left = {"fs": rem4(z + 3) * 4 + y, "tp": tp}
    partner = {"fs": fs, "tp": x * 2 + 1 - c}

    rows = og_hbm.shape[0]
    half = rows // 2
    ff, cols = dw_hbm.shape
    wide = 4 * cols
    quarter = ff // 4
    urows = uw_hbm.shape[0]
    tokens = pg.shape[0]

    line = 2 * og.shape[1]
    w = Wires(send_sem, recv_sem, partner, lambda size: og.at[pl.ds(0, size // line), :])

    def token_rows(ref, block):
        return ref.at[pl.ds(pl.multiple_of(block * rows, rows), rows), :]

    def lanes(i):
        return pl.ds(pl.multiple_of(i * cols, cols), cols)

    mine = [
        (dw_hbm, wd.at[z, :, lanes(y)]),
        (og_hbm, token_rows(og, tp)),
        (uw_hbm, wu.at[z, y]),
        (pa_hbm, pg),
        (ni_hbm, token_rows(ni, tp)),
    ]
    local = [
        pltpu.make_async_copy(src, dst, local_sem.at[i])
        for i, (src, dst) in enumerate(mine)
    ]
    barrier = pltpu.get_barrier_semaphore()
    for device in (x_right, x_left, y_right, y_left, z_right, z_left, partner):
        pl.semaphore_signal(barrier, inc=1, device_id=device, device_id_type=MESH)
    for copy in local:
        copy.start()
    pl.semaphore_wait(barrier, 7)

    def wd_rows(p):
        return pl.ds(p * quarter, quarter)

    def wu_rows(p):
        return pl.ds(p * (urows // 4), urows // 4)

    def weight_rings(tag, one, z_group, y_group):
        return (
            (
                Gather(w, tag, tag + "a1", y, y_right, y_left, lambda i, p: one(z, i, p)),
                Gather(w, tag, tag + "b1", z, z_right, z_left, lambda i, p: one(i, y, 2 + p)),
            ),
            (
                Gather(w, tag, tag + "a2", z, z_right, z_left, lambda i, p: z_group(i, p)),
                Gather(w, tag, tag + "b2", y, y_right, y_left, lambda i, p: y_group(i, 2 + p)),
            ),
        )

    wd1, _ = weight_rings(
        "d",
        lambda zi, yi, p: wd.at[zi, wd_rows(p), lanes(yi)],
        lambda zi, p: wd.at[zi, wd_rows(p), :],
        lambda yi, p: wd.at[:, wd_rows(p), lanes(yi)],
    )
    wd2 = (
        QuarterGather(
            w, "d", "da2", z, z_right, z_left,
            lambda i, p: wd.at[i, wd_rows(p), :],
            lambda i, p, h: wd.at[i, wd_rows(p), lanes(rem4(y + h))],
        ),
        QuarterGather(
            w, "d", "db2", y, y_right, y_left,
            lambda i, p: wd.at[:, wd_rows(2 + p), lanes(i)],
            lambda i, p, h: wd.at[rem4(z + h), wd_rows(2 + p), lanes(i)],
        ),
    )
    wu1, wu2 = weight_rings(
        "u",
        lambda zi, yi, p: wu.at[zi, yi, wu_rows(p), :],
        lambda zi, p: wu.at[zi, :, wu_rows(p), :],
        lambda yi, p: wu.at[:, yi, wu_rows(p), :],
    )

    for pair in (wd1, wd2, wu1, wu2):
        paired(*pair)

    def token_piece(ref, core):
        def piece(i, p):
            start = pl.multiple_of((i * 2 + core) * rows + p * half, half)
            return ref.at[pl.ds(start, half), :]

        return piece

    rings = {
        "o": Gather(w, "o", "o", x, x_right, x_left, token_piece(og, c)),
        "n": Gather(w, "n", "n", x, x_right, x_left, token_piece(ni, c)),
    }

    def hand(tag, *pieces):
        for hop, p in pieces:
            ref = rings[tag].at(hop, p)
            w.send(tag, (tag, "cross"), ref, ref, partner)

    def handed(tag):
        w.recv((tag, "cross"), 8 * rings[tag].size)

    def token_own(tag):
        rings[tag].own()
        hand(tag, (0, 0), (0, 1))

    def token_forward(tag):
        rings[tag].forward()
        hand(tag, (3, 0), (1, 1))

    def token_near(tag):
        rings[tag].near()
        hand(tag, (3, 1), (1, 0))

    def token_far(tag):
        rings[tag].far()
        hand(tag, (2, 0), (2, 1))

    def each(pair, step):
        for ring in pair:
            getattr(ring, step)()

    def hidden(count, first):
        def body(j, carry):
            at = pl.multiple_of(j * 128, 128)
            active = jnp.maximum(pg[pl.ds(at, 128), :].astype(F32), 0.0)
            ht[:, pl.ds(at, 128)] = (active * active).astype(BF16).T
            return carry

        lax.fori_loop(first, first + count, body, 0)

    def give(pair, *what):
        for ring in pair:
            ring.give(*what)

    local[0].wait()
    each(wd1, "own")
    local[1].wait()
    token_own("o")
    local[2].wait()
    each(wu1, "own")
    give(wd2, 0, 0)
    give(wd2, 1, 0)
    local[3].wait()
    hidden(6, 0)
    each(wd1, "forward")
    each(wu1, "forward")
    hidden(6, 6)
    each(wd1, "near")
    give(wd2, 0, 1, 3)
    token_forward("o")
    each(wd1, "far")
    give(wd2, 0, 2)
    give(wd2, 1, 1, 3, 2)
    local[4].wait()
    token_own("n")
    each(wu1, "near")
    each(wu1, "far")
    each(wd2, "forward")
    each(wu2, "own")
    token_near("o")
    token_far("o")
    each(wd2, "near")
    each(wd2, "far")
    handed("o")

    block = 256

    def pre_grad(i, carry):
        at = pl.ds(pl.multiple_of(i * block, block), block)
        for n in range(2):
            units = pl.ds(n * ff // 2, ff // 2)
            weight = jnp.concatenate([wd[k, units, :] for k in range(4)], axis=1)
            grad = nt(og[at, :], weight)
            active = jnp.maximum(pg[at, units].astype(F32), 0.0)
            value = (2.0 * active * grad).astype(BF16)
            pg[at, units] = value
            pgt[units, at] = value.T

        @pl.when(i == 3)
        def _():
            each(wu2, "forward")

        @pl.when(i == 5)
        def _():
            token_forward("n")

        return carry

    lax.fori_loop(0, tokens // block, pre_grad, 0)

    def grad_rings(tag, grad, zland, yland, yone, zone):
        return (
            (
                Scatter(
                    w, tag, tag + "a1", z, z_right, z_left,
                    lambda i, p: grad.at[i, wd_rows(p), :],
                    lambda side, m: zland.at[side, m],
                ),
                Scatter(
                    w, tag, tag + "b1", y, y_right, y_left,
                    lambda i, p: grad.at[:, wd_rows(2 + p), lanes(i)],
                    lambda side, m: yland.at[side, m],
                ),
            ),
            (
                Scatter(
                    w, tag, tag + "a2", y, y_right, y_left,
                    lambda i, p: grad.at[z, wd_rows(p), lanes(i)],
                    lambda side, m: yone.at[side, m],
                ),
                Scatter(
                    w, tag, tag + "b2", z, z_right, z_left,
                    lambda i, p: grad.at[i, wd_rows(2 + p), lanes(y)],
                    lambda side, m: zone.at[side, m],
                ),
            ),
        )

    gd1, gd2 = grad_rings("D", gd, zland_d, yland_d, yone_d, zone_d)
    gu = wd
    _, gu2 = grad_rings("U", gu, zland_u, yland_u, yone_u, zone_u)
    gu1 = (
        QuarterScatter(
            w, "U", "Ua1", z, z_right, z_left,
            lambda i, p: gu.at[i, wd_rows(p), :],
            lambda side, m: zland_u.at[side, m],
            lambda i, p, h: gu.at[i, wd_rows(p), lanes(rem4(y + h))],
            lambda side, m, h: zland_u.at[side, m, :, lanes(rem4(y + h))],
        ),
        QuarterScatter(
            w, "U", "Ub1", y, y_right, y_left,
            lambda i, p: gu.at[:, wd_rows(2 + p), lanes(i)],
            lambda side, m: yland_u.at[side, m],
            lambda i, p, h: gu.at[rem4(z + h), wd_rows(2 + p), lanes(i)],
            lambda side, m, h: yland_u.at[side, m, rem4(z + h)],
        ),
    )
    for pair in (gd1, gd2, gu1, gu2):
        paired(*pair)
    upper = ff // 2

    def hop_of(k):
        return jnp.where(k == 0, 2, jnp.where(k == 1, 1, jnp.where(k == 2, 3, 0)))

    def weight_grad(left, right, grad, first, extra):
        def body(k, carry):
            zi, yi = rem4(z + hop_of(k)), rem4(y + hop_of(k))
            strip = right[:, pl.ds(pl.multiple_of(zi * wide, wide), wide)]
            grad[zi, :upper, :] = nn(left[:upper, :], strip).astype(BF16)
            strip = jnp.concatenate(
                [right[:, pl.ds(pl.multiple_of(g * wide + yi * cols, cols), cols)] for g in range(4)],
                axis=1,
            )
            value = nn(left[upper:, :], strip).astype(BF16)
            for g in range(4):
                grad[g, upper:, lanes(yi)] = value[:, g * cols : (g + 1) * cols]

            if extra:
                extra(k)
            for turn, step in ((0, "far"), (1, "to_right"), (2, "to_left")):

                @pl.when(k == turn)
                def _(step=step):
                    each(first, step)

            return carry

        lax.fori_loop(0, 4, body, 0)

    weight_grad(ht, og, gd, gd1, None)

    each(wu2, "near")
    each(wu2, "far")

    def share(block):
        return part.at[block]

    xs = Scatter(
        w, "x", "x", x, x_right, x_left,
        lambda i, p: part.at[i * 2 + c, pl.ds(p * half, half), :],
        lambda side, m: xland.at[side, m],
    )
    cross_base = [w.key(("c", k)) for k in range(4)][0]
    cross_group = w.group("c")
    w.bytes["c"] = size_of(cross)

    def product(xi):
        at = pl.ds(pl.multiple_of(xi * 2 * rows, 2 * rows), 2 * rows)
        for g in range(4):
            value = nt(pg[at, :], wu[g].reshape(4 * urows, ff)).astype(BF16)
            out = pl.ds(g * 4 * urows, 4 * urows)
            part[xi * 2, :, out] = value[:rows]
            part[xi * 2 + 1, :, out] = value[rows:]

    def send_cross(k):
        block = part.at[rem4(x + hop_of(k)) * 2 + 1 - c]
        w.copy(cross_group, cross_base + k, block, cross.at[k], partner).start()

    def add_cross(k):
        index = rem4(x + hop_of(k)) * 2 + c
        w.copy(cross_group, cross_base + k, cross.at[k], cross.at[k], partner).wait_recv()
        total = part[index].astype(F32) + cross[k].astype(F32)
        part[index] = total.astype(BF16)

    def input_grad(k, carry):
        xi = rem4(x + hop_of(k))
        product(xi)
        send_cross(k)

        @pl.when(k == 0)
        def _():
            token_near("n")

        @pl.when(k == 1)
        def _():
            each(gd1, "middle")
            add_cross(0)
            xs.far()

        @pl.when(k == 2)
        def _():
            token_far("n")
            add_cross(1)
            xs.to_right()

        return carry

    lax.fori_loop(0, 3, input_grad, 0)
    handed("n")
    w.drain("d")

    def while_up(k):
        @pl.when(k == 0)
        def _():
            add_cross(2)
            xs.to_left()

        @pl.when(k == 1)
        def _():
            each(gd1, "finish")
            each(gd2, "far")
            each(gd2, "to_right")
            each(gd2, "to_left")

        @pl.when(k == 2)
        def _():
            xs.middle()

    weight_grad(pgt, ni, gu, gu1, while_up)

    product(x)
    send_cross(3)
    each(gu1, "add_first")
    give(gu1, 2, 1, 3)
    each(gd2, "middle")
    add_cross(3)

    def settle(h):
        for ring in gu1:
            ring.settle(h)

    each(gu1, "settle_near")
    settle(2)
    each(gu2, "far")
    give(gu1, 0)
    settle(1)
    each(gu2, "to_right")
    settle(3)
    each(gu2, "to_left")

    each(gu2, "middle")
    settle(0)

    def store_rows(p, total):
        ig[pl.ds(p * half, half), :] = total.astype(BF16)

    xs.finish(store_rows)
    for i, ring in enumerate(gd2):

        def store_down(p, total, i=i):
            dg[wd_rows(2 * i + p), :] = total

        ring.finish(store_down)
    for i, ring in enumerate(gu2):

        def store_up(p, total, i=i):
            ug[:, wd_rows(2 * i + p)] = total.T

        ring.finish(store_up)
    for group in ("u", "o", "n", "D", "U", "x", "c"):
        w.drain(group)


def deliver(*refs):
    sem = refs[-1]
    copies = [pltpu.make_async_copy(refs[i], refs[3 + i], sem.at[i]) for i in range(3)]
    for copy in copies:
        copy.start()
    for copy in copies:
        copy.wait()


def local(normed_input, pre_act, out_grad, up_weight, down_weight):
    rows, d = out_grad.shape
    tokens, ff = pre_act.shape
    cols = down_weight.shape[1]
    quarter = ff // 4
    half = rows // 2
    grads = [
        pltpu.VMEM((2, 3, quarter, 4 * cols), BF16),
        pltpu.VMEM((2, 3, 4, quarter, cols), BF16),
        pltpu.VMEM((2, 3, quarter, cols), BF16),
        pltpu.VMEM((2, 3, quarter, cols), BF16),
    ]
    input_grad, up_grad, down_grad = pl.pallas_call(
        kernel,
        out_shape=(
            pltpu.VMEM((rows, d), BF16),
            pltpu.VMEM((cols, ff), F32),
            pltpu.VMEM((ff, cols), F32),
        ),
        in_specs=[pl.BlockSpec(memory_space=pltpu.HBM)] * 5,
        out_specs=(pl.BlockSpec(memory_space=pltpu.VMEM),) * 3,
        scratch_shapes=[
            pltpu.VMEM((tokens, d), BF16),
            pltpu.VMEM((tokens, d), BF16),
            pltpu.VMEM((4, ff, 4 * cols), BF16),
            pltpu.VMEM((4, 4, d // 16, ff), BF16),
            pltpu.VMEM((tokens, ff), BF16),
            pltpu.VMEM((ff, tokens), BF16),
            pltpu.VMEM((ff, tokens), BF16),
            pltpu.VMEM((8, rows, d), BF16),
            pltpu.VMEM((4, ff, 4 * cols), BF16),
            pltpu.VMEM((4, rows, d), BF16),
            pltpu.VMEM((2, 3, half, d), BF16),
            *grads,
            *grads,
            pltpu.SemaphoreType.DMA((SENDS,)),
            pltpu.SemaphoreType.DMA((RECVS,)),
            pltpu.SemaphoreType.DMA((5,)),
        ],
        compiler_params=pltpu.CompilerParams(
            collective_id=0,
            has_side_effects=True,
            vmem_limit_bytes=62800000,
        ),
        name="ffn_backward",
    )(normed_input, pre_act, out_grad, up_weight, down_weight)
    return pl.pallas_call(
        deliver,
        out_shape=(
            jax.ShapeDtypeStruct((rows, d), BF16),
            jax.ShapeDtypeStruct((cols, ff), F32),
            jax.ShapeDtypeStruct((ff, cols), F32),
        ),
        in_specs=[pl.BlockSpec(memory_space=pl.ANY)] * 3,
        out_specs=(pl.BlockSpec(memory_space=pl.ANY),) * 3,
        scratch_shapes=[pltpu.SemaphoreType.DMA((3,))],
        compiler_params=pltpu.CompilerParams(vmem_limit_bytes=4 * 2**20),
        name="deliver",
    )(input_grad, up_grad, down_grad)


def solution(mesh):
    placed = (
        P(("fs", "tp"), None),
        P("fs", "tp"),
        P(("fs", "tp"), None),
        P("fs", "tp"),
        P("tp", "fs"),
    )
    return jax.shard_map(
        local,
        mesh=mesh,
        in_specs=placed,
        out_specs=(P(("fs", "tp"), None), P("fs", "tp"), P("tp", "fs")),
        check_vma=False,
    )
```

```python
import math

import jax
import jax.numpy as jnp
from jax import lax
from jax.experimental import pallas as pl
from jax.experimental.pallas import tpu as pltpu
from jax.sharding import PartitionSpec as P

MESH = pl.DeviceIdType.MESH
F32 = jnp.float32
BF16 = jnp.bfloat16
SENDS, RECVS = 8, 38


def rem4(value):
    return lax.rem(value, 4)


def nt(a, b):
    return lax.dot_general(a, b, (((1,), (1,)), ((), ())), preferred_element_type=F32)


def nn(a, b):
    return jnp.dot(a, b, preferred_element_type=F32)


def size_of(ref):
    return 2 * math.prod(ref.shape)


class Wires:
    def __init__(self, send_sem, recv_sem, partner, filler):
        self.send_sem, self.recv_sem, self.partner = send_sem, recv_sem, partner
        self.filler = filler
        self.groups, self.keys, self.bytes = {}, {}, {}

    def group(self, name):
        return self.groups.setdefault(name, len(self.groups))

    def key(self, name):
        return self.keys.setdefault(name, len(self.keys))

    def copy(self, g, k, src, dst, device):
        return pltpu.make_async_remote_copy(
            src_ref=src,
            dst_ref=dst,
            send_sem=self.send_sem.at[g],
            recv_sem=self.recv_sem.at[k],
            device_id=device,
            device_id_type=MESH,
        )

    def send(self, group, key, src, dst, device):
        self.copy(self.group(group), self.key(key), src, dst, device).start()
        self.bytes[group] = self.bytes.get(group, 0) + size_of(src)

    def recv(self, key, size):
        ref = self.filler(size)
        self.copy(0, self.key(key), ref, ref, self.partner).wait_recv()

    def drain(self, group):
        ref = self.filler(self.bytes[group])
        self.copy(self.group(group), 0, ref, ref, self.partner).wait_send()


class Gather:
    share = 1

    def __init__(self, wires, group, tag, pos, right, left, piece):
        self.w, self.group, self.tag, self.pos = wires, group, tag, pos
        self.right, self.left, self.piece = right, left, piece
        self.size = size_of(piece(pos, 0))

    def wait(self, name, pieces):
        if self.share:
            self.w.recv((self.tag, name), self.share * pieces * self.size)

    def at(self, hop, p):
        return self.piece(rem4(self.pos + hop), p)

    def put(self, name, hop, p, device):
        ref = self.at(hop, p)
        self.w.send(self.group, (self.tag, name), ref, ref, device)

    def own(self):
        self.put("first", 0, 0, self.right)
        self.put("first", 0, 1, self.left)
        self.put("near", 0, 1, self.right)
        self.put("near", 0, 0, self.left)

    def forward(self):
        self.wait("first", 2)
        self.put("far", 3, 0, self.right)
        self.put("far", 1, 1, self.left)

    def near(self):
        self.wait("near", 2)

    def far(self):
        self.wait("far", 2)


class QuarterGather(Gather):
    def __init__(self, wires, group, tag, pos, right, left, piece, quarter):
        super().__init__(wires, group, tag, pos, right, left, piece)
        self.quarter = quarter

    def give(self, turn, *members):
        name = (self.tag, "near" if turn else "first")
        for h in members:
            for device, p in ((self.right, turn), (self.left, 1 - turn)):
                ref = self.quarter(self.pos, p, h)
                self.w.send(self.group, name, ref, ref, device)


class Scatter:
    share = 1

    def __init__(self, wires, group, tag, pos, right, left, piece, landing):
        self.w, self.group, self.tag, self.pos = wires, group, tag, pos
        self.right, self.left = right, left
        self.piece, self.landing = piece, landing
        self.size = size_of(piece(pos, 0))

    def wait(self, name, quarters):
        if self.share:
            self.w.recv((self.tag, name), self.share * quarters * self.size // 4)

    def at(self, hop, p):
        return self.piece(rem4(self.pos + hop), p)

    def put(self, name, side, m, hop, p):
        self.w.send(
            self.group,
            (self.tag, name),
            self.at(hop, p),
            self.landing(side, m),
            self.right if side == 0 else self.left,
        )

    def far(self):
        self.put("first", 0, 0, 2, 0)
        self.put("first", 1, 0, 2, 1)

    def to_right(self):
        self.put("last", 0, 1, 1, 1)

    def to_left(self):
        self.put("last", 1, 1, 3, 0)

    def add_first(self):
        self.wait("first", 8)
        for side, hop, p in ((0, 1, 0), (1, 3, 1)):
            came, mine = self.landing(side, 0), self.at(hop, p)
            mine[...] = (mine[...].astype(F32) + came[...].astype(F32)).astype(BF16)

    def middle(self):
        self.add_first()
        self.put("last", 0, 2, 1, 0)
        self.put("last", 1, 2, 3, 1)

    def finish(self, store=None):
        self.wait("last", 16)
        for p, near, far in ((1, 0, 1), (0, 1, 0)):
            first, second = self.landing(near, 1), self.landing(far, 2)
            mine = self.at(0, p)
            total = mine[...].astype(F32) + first[...].astype(F32) + second[...].astype(F32)
            if store is None:
                mine[...] = total.astype(BF16)
            else:
                store(p, total)


class QuarterScatter(Scatter):
    def __init__(self, wires, group, tag, pos, right, left, piece, landing, quarter, landed):
        super().__init__(wires, group, tag, pos, right, left, piece, landing)
        self.quarter, self.landed = quarter, landed

    def give(self, *members):
        for h in members:
            for side, hop, p in ((0, 1, 0), (1, 3, 1)):
                self.w.send(
                    self.group,
                    (self.tag, h),
                    self.quarter(rem4(self.pos + hop), p, h),
                    self.landed(side, 2, h),
                    self.right if side == 0 else self.left,
                )

    def near(self, *members):
        for h in members:
            for side, hop, p in ((0, 1, 1), (1, 3, 0)):
                self.w.send(
                    self.group,
                    (self.tag, h),
                    self.quarter(rem4(self.pos + hop), p, h),
                    self.landed(side, 1, h),
                    self.right if side == 0 else self.left,
                )

    def settle(self, h):
        self.wait(h, 4)
        for p, near, far in ((1, 0, 1), (0, 1, 0)):
            first, second = self.landed(near, 1, h), self.landed(far, 2, h)
            mine = self.quarter(self.pos, p, h)
            total = mine[...].astype(F32) + first[...].astype(F32) + second[...].astype(F32)
            mine[...] = total.astype(BF16)


def paired(first, second):
    second.tag, first.share, second.share = first.tag, 2, 0
    return first, second


def kernel(
    ni_hbm, pa_hbm, og_hbm, uw_hbm, dw_hbm,
    ig, ug, dg,
    ni, og, wd, wu, pg, ht, pgt, part, gd,
    cross, xland, zland_d, yland_d, yone_d, zone_d,
    zland_u, yland_u, yone_u, zone_u,
    send_sem, recv_sem, local_sem,
):
    fs, tp = lax.axis_index("fs"), lax.axis_index("tp")
    z, y, x, c = fs // 4, rem4(fs), tp // 2, lax.rem(tp, 2)
    x_right = {"fs": fs, "tp": rem4(x + 1) * 2 + c}
    x_left = {"fs": fs, "tp": rem4(x + 3) * 2 + c}
    y_right = {"fs": z * 4 + rem4(y + 1), "tp": tp}
    y_left = {"fs": z * 4 + rem4(y + 3), "tp": tp}
    z_right = {"fs": rem4(z + 1) * 4 + y, "tp": tp}
    z_left = {"fs": rem4(z + 3) * 4 + y, "tp": tp}
    partner = {"fs": fs, "tp": x * 2 + 1 - c}

    rows = og_hbm.shape[0]
    half = rows // 2
    ff, cols = dw_hbm.shape
    wide = 4 * cols
    quarter = ff // 4
    urows = uw_hbm.shape[0]
    tokens = pg.shape[0]

    line = 2 * og.shape[1]
    w = Wires(send_sem, recv_sem, partner, lambda size: og.at[pl.ds(0, size // line), :])

    def token_rows(ref, block):
        return ref.at[pl.ds(pl.multiple_of(block * rows, rows), rows), :]

    def lanes(i):
        return pl.ds(pl.multiple_of(i * cols, cols), cols)

    mine = [
        (dw_hbm, wd.at[z, :, lanes(y)]),
        (og_hbm, token_rows(og, tp)),
        (uw_hbm, wu.at[z, y]),
        (pa_hbm, pg),
        (ni_hbm, token_rows(ni, tp)),
    ]
    local = [
        pltpu.make_async_copy(src, dst, local_sem.at[i])
        for i, (src, dst) in enumerate(mine)
    ]
    barrier = pltpu.get_barrier_semaphore()
    for device in (x_right, x_left, y_right, y_left, z_right, z_left, partner):
        pl.semaphore_signal(barrier, inc=1, device_id=device, device_id_type=MESH)
    for copy in local:
        copy.start()
    pl.semaphore_wait(barrier, 7)

    def wd_rows(p):
        return pl.ds(p * quarter, quarter)

    def wu_rows(p):
        return pl.ds(p * (urows // 4), urows // 4)

    def weight_rings(tag, one, z_group, y_group):
        return (
            (
                Gather(w, tag, tag + "a1", y, y_right, y_left, lambda i, p: one(z, i, p)),
                Gather(w, tag, tag + "b1", z, z_right, z_left, lambda i, p: one(i, y, 2 + p)),
            ),
            (
                Gather(w, tag, tag + "a2", z, z_right, z_left, lambda i, p: z_group(i, p)),
                Gather(w, tag, tag + "b2", y, y_right, y_left, lambda i, p: y_group(i, 2 + p)),
            ),
        )

    wd1, _ = weight_rings(
        "d",
        lambda zi, yi, p: wd.at[zi, wd_rows(p), lanes(yi)],
        lambda zi, p: wd.at[zi, wd_rows(p), :],
        lambda yi, p: wd.at[:, wd_rows(p), lanes(yi)],
    )
    wd2 = (
        QuarterGather(
            w, "d", "da2", z, z_right, z_left,
            lambda i, p: wd.at[i, wd_rows(p), :],
            lambda i, p, h: wd.at[i, wd_rows(p), lanes(rem4(y + h))],
        ),
        QuarterGather(
            w, "d", "db2", y, y_right, y_left,
            lambda i, p: wd.at[:, wd_rows(2 + p), lanes(i)],
            lambda i, p, h: wd.at[rem4(z + h), wd_rows(2 + p), lanes(i)],
        ),
    )
    wu1, wu2 = weight_rings(
        "u",
        lambda zi, yi, p: wu.at[zi, yi, wu_rows(p), :],
        lambda zi, p: wu.at[zi, :, wu_rows(p), :],
        lambda yi, p: wu.at[:, yi, wu_rows(p), :],
    )

    for pair in (wd1, wd2, wu1, wu2):
        paired(*pair)

    def token_piece(ref, core):
        def piece(i, p):
            start = pl.multiple_of((i * 2 + core) * rows + p * half, half)
            return ref.at[pl.ds(start, half), :]

        return piece

    rings = {
        "o": Gather(w, "o", "o", x, x_right, x_left, token_piece(og, c)),
        "n": Gather(w, "n", "n", x, x_right, x_left, token_piece(ni, c)),
    }

    def hand(tag, *pieces):
        for hop, p in pieces:
            ref = rings[tag].at(hop, p)
            w.send(tag, (tag, "cross"), ref, ref, partner)

    def handed(tag):
        w.recv((tag, "cross"), 8 * rings[tag].size)

    def token_own(tag):
        rings[tag].own()
        hand(tag, (0, 0), (0, 1))

    def token_forward(tag):
        rings[tag].forward()
        hand(tag, (3, 0), (1, 1))

    def token_near(tag):
        rings[tag].near()
        hand(tag, (3, 1), (1, 0))

    def token_far(tag):
        rings[tag].far()
        hand(tag, (2, 0), (2, 1))

    def each(pair, step):
        for ring in pair:
            getattr(ring, step)()

    def hidden(count, first):
        def body(j, carry):
            at = pl.multiple_of(j * 128, 128)
            active = jnp.maximum(pg[pl.ds(at, 128), :].astype(F32), 0.0)
            ht[:, pl.ds(at, 128)] = (active * active).astype(BF16).T
            return carry

        lax.fori_loop(first, first + count, body, 0)

    def give(pair, *what):
        for ring in pair:
            ring.give(*what)

    local[0].wait()
    each(wd1, "own")
    local[1].wait()
    token_own("o")
    local[2].wait()
    each(wu1, "own")
    give(wd2, 0, 0)
    give(wd2, 1, 0)
    local[3].wait()
    hidden(6, 0)
    each(wd1, "forward")
    each(wu1, "forward")
    hidden(6, 6)
    each(wd1, "near")
    give(wd2, 0, 1, 3)
    token_forward("o")
    each(wd1, "far")
    give(wd2, 0, 2)
    give(wd2, 1, 1, 3, 2)
    local[4].wait()
    token_own("n")
    each(wu1, "near")
    each(wu1, "far")
    each(wd2, "forward")
    each(wu2, "own")
    token_near("o")
    token_far("o")
    each(wd2, "near")
    each(wd2, "far")
    handed("o")

    block = 256

    def pre_grad(i, carry):
        at = pl.ds(pl.multiple_of(i * block, block), block)
        for n in range(2):
            units = pl.ds(n * ff // 2, ff // 2)
            weight = jnp.concatenate([wd[k, units, :] for k in range(4)], axis=1)
            grad = nt(og[at, :], weight)
            active = jnp.maximum(pg[at, units].astype(F32), 0.0)
            value = (2.0 * active * grad).astype(BF16)
            pg[at, units] = value
            pgt[units, at] = value.T

        @pl.when(i == 2)
        def _():
            each(wu2, "forward")

        @pl.when(i == 5)
        def _():
            token_forward("n")

        return carry

    lax.fori_loop(0, tokens // block, pre_grad, 0)

    def grad_rings(tag, grad, zland, yland, yone, zone):
        return (
            (
                Scatter(
                    w, tag, tag + "a1", z, z_right, z_left,
                    lambda i, p: grad.at[i, wd_rows(p), :],
                    lambda side, m: zland.at[side, m],
                ),
                Scatter(
                    w, tag, tag + "b1", y, y_right, y_left,
                    lambda i, p: grad.at[:, wd_rows(2 + p), lanes(i)],
                    lambda side, m: yland.at[side, m],
                ),
            ),
            (
                Scatter(
                    w, tag, tag + "a2", y, y_right, y_left,
                    lambda i, p: grad.at[z, wd_rows(p), lanes(i)],
                    lambda side, m: yone.at[side, m],
                ),
                Scatter(
                    w, tag, tag + "b2", z, z_right, z_left,
                    lambda i, p: grad.at[i, wd_rows(2 + p), lanes(y)],
                    lambda side, m: zone.at[side, m],
                ),
            ),
        )

    gd1, gd2 = grad_rings("D", gd, zland_d, yland_d, yone_d, zone_d)
    gu = wd
    _, gu2 = grad_rings("U", gu, zland_u, yland_u, yone_u, zone_u)
    gu1 = (
        QuarterScatter(
            w, "U", "Ua1", z, z_right, z_left,
            lambda i, p: gu.at[i, wd_rows(p), :],
            lambda side, m: zland_u.at[side, m],
            lambda i, p, h: gu.at[i, wd_rows(p), lanes(rem4(y + h))],
            lambda side, m, h: zland_u.at[side, m, :, lanes(rem4(y + h))],
        ),
        QuarterScatter(
            w, "U", "Ub1", y, y_right, y_left,
            lambda i, p: gu.at[:, wd_rows(2 + p), lanes(i)],
            lambda side, m: yland_u.at[side, m],
            lambda i, p, h: gu.at[rem4(z + h), wd_rows(2 + p), lanes(i)],
            lambda side, m, h: yland_u.at[side, m, rem4(z + h)],
        ),
    )
    for pair in (gd1, gd2, gu1, gu2):
        paired(*pair)
    upper = ff // 2

    def hop_of(k):
        return jnp.where(k == 0, 2, jnp.where(k == 1, 1, jnp.where(k == 2, 3, 0)))

    def weight_grad(left, right, grad, first, steps, extra):
        def body(k, carry):
            zi, yi = rem4(z + hop_of(k)), rem4(y + hop_of(k))
            strip = right[:, pl.ds(pl.multiple_of(zi * wide, wide), wide)]
            grad[zi, :upper, :] = nn(left[:upper, :], strip).astype(BF16)
            strip = jnp.concatenate(
                [right[:, pl.ds(pl.multiple_of(g * wide + yi * cols, cols), cols)] for g in range(4)],
                axis=1,
            )
            value = nn(left[upper:, :], strip).astype(BF16)
            for g in range(4):
                grad[g, upper:, lanes(yi)] = value[:, g * cols : (g + 1) * cols]

            if extra:
                extra(k)
            for turn, step in enumerate(steps):

                @pl.when(k == turn)
                def _(step=step):
                    each(first, step)

            return carry

        lax.fori_loop(0, 4, body, 0)

    weight_grad(ht, og, gd, gd1, ("far", "to_right", "to_left"), None)

    each(wu2, "near")
    each(wu2, "far")

    def share(block):
        return part.at[block]

    xs = Scatter(
        w, "x", "x", x, x_right, x_left,
        lambda i, p: part.at[i * 2 + c, pl.ds(p * half, half), :],
        lambda side, m: xland.at[side, m],
    )
    cross_base = [w.key(("c", k)) for k in range(4)][0]
    cross_group = w.group("c")
    w.bytes["c"] = size_of(cross)

    def product(xi):
        at = pl.ds(pl.multiple_of(xi * 2 * rows, 2 * rows), 2 * rows)
        for g in range(4):
            value = nt(pg[at, :], wu[g].reshape(4 * urows, ff)).astype(BF16)
            out = pl.ds(g * 4 * urows, 4 * urows)
            part[xi * 2, :, out] = value[:rows]
            part[xi * 2 + 1, :, out] = value[rows:]

    def send_cross(k):
        block = part.at[rem4(x + hop_of(k)) * 2 + 1 - c]
        w.copy(cross_group, cross_base + k, block, cross.at[k], partner).start()

    def add_cross(k):
        index = rem4(x + hop_of(k)) * 2 + c
        w.copy(cross_group, cross_base + k, cross.at[k], cross.at[k], partner).wait_recv()
        total = part[index].astype(F32) + cross[k].astype(F32)
        part[index] = total.astype(BF16)

    def input_grad(k, carry):
        xi = rem4(x + hop_of(k))
        product(xi)

        @pl.when(k == 2)
        def _():
            token_far("n")

        send_cross(k)

        @pl.when(k == 0)
        def _():
            token_near("n")

        @pl.when(k == 1)
        def _():
            each(gd1, "middle")
            add_cross(0)
            xs.far()

        @pl.when(k == 2)
        def _():
            add_cross(1)
            xs.to_right()

        return carry

    lax.fori_loop(0, 3, input_grad, 0)
    handed("n")
    w.drain("d")

    def near(*members):
        for ring in gu1:
            ring.near(*members)

    def while_up(k):
        @pl.when(k == 0)
        def _():
            add_cross(2)
            xs.to_left()

        @pl.when(k == 1)
        def _():
            each(gd1, "finish")
            each(gd2, "far")
            each(gd2, "to_right")
            each(gd2, "to_left")

        @pl.when(k == 2)
        def _():
            near(2)
            xs.middle()

    weight_grad(pgt, ni, gu, gu1, ("far",), while_up)

    def settle(h):
        for ring in gu1:
            ring.settle(h)

    near(1)
    each(gu1, "add_first")
    give(gu1, 2, 1)
    near(3)
    give(gu1, 3)
    product(x)
    send_cross(3)
    each(gd2, "middle")
    settle(2)
    each(gu2, "far")
    near(0)
    give(gu1, 0)
    settle(1)
    each(gu2, "to_right")
    settle(3)
    each(gu2, "to_left")
    add_cross(3)
    each(gu2, "middle")
    settle(0)

    def store_rows(p, total):
        ig[pl.ds(p * half, half), :] = total.astype(BF16)

    xs.finish(store_rows)
    for i, ring in enumerate(gd2):

        def store_down(p, total, i=i):
            dg[wd_rows(2 * i + p), :] = total

        ring.finish(store_down)
    for i, ring in enumerate(gu2):

        def store_up(p, total, i=i):
            ug[:, wd_rows(2 * i + p)] = total.T

        ring.finish(store_up)
    for group in ("u", "o", "n", "D", "U", "x", "c"):
        w.drain(group)


def deliver(*refs):
    sem = refs[-1]
    copies = [pltpu.make_async_copy(refs[i], refs[3 + i], sem.at[i]) for i in range(3)]
    for copy in copies:
        copy.start()
    for copy in copies:
        copy.wait()


def local(normed_input, pre_act, out_grad, up_weight, down_weight):
    rows, d = out_grad.shape
    tokens, ff = pre_act.shape
    cols = down_weight.shape[1]
    quarter = ff // 4
    half = rows // 2
    grads = [
        pltpu.VMEM((2, 3, quarter, 4 * cols), BF16),
        pltpu.VMEM((2, 3, 4, quarter, cols), BF16),
        pltpu.VMEM((2, 3, quarter, cols), BF16),
        pltpu.VMEM((2, 3, quarter, cols), BF16),
    ]
    input_grad, up_grad, down_grad = pl.pallas_call(
        kernel,
        out_shape=(
            pltpu.VMEM((rows, d), BF16),
            pltpu.VMEM((cols, ff), F32),
            pltpu.VMEM((ff, cols), F32),
        ),
        in_specs=[pl.BlockSpec(memory_space=pltpu.HBM)] * 5,
        out_specs=(pl.BlockSpec(memory_space=pltpu.VMEM),) * 3,
        scratch_shapes=[
            pltpu.VMEM((tokens, d), BF16),
            pltpu.VMEM((tokens, d), BF16),
            pltpu.VMEM((4, ff, 4 * cols), BF16),
            pltpu.VMEM((4, 4, d // 16, ff), BF16),
            pltpu.VMEM((tokens, ff), BF16),
            pltpu.VMEM((ff, tokens), BF16),
            pltpu.VMEM((ff, tokens), BF16),
            pltpu.VMEM((8, rows, d), BF16),
            pltpu.VMEM((4, ff, 4 * cols), BF16),
            pltpu.VMEM((4, rows, d), BF16),
            pltpu.VMEM((2, 3, half, d), BF16),
            *grads,
            *grads,
            pltpu.SemaphoreType.DMA((SENDS,)),
            pltpu.SemaphoreType.DMA((RECVS,)),
            pltpu.SemaphoreType.DMA((5,)),
        ],
        compiler_params=pltpu.CompilerParams(
            collective_id=0,
            has_side_effects=True,
            vmem_limit_bytes=62800000,
        ),
        name="ffn_backward",
    )(normed_input, pre_act, out_grad, up_weight, down_weight)
    return pl.pallas_call(
        deliver,
        out_shape=(
            jax.ShapeDtypeStruct((rows, d), BF16),
            jax.ShapeDtypeStruct((cols, ff), F32),
            jax.ShapeDtypeStruct((ff, cols), F32),
        ),
        in_specs=[pl.BlockSpec(memory_space=pl.ANY)] * 3,
        out_specs=(pl.BlockSpec(memory_space=pl.ANY),) * 3,
        scratch_shapes=[pltpu.SemaphoreType.DMA((3,))],
        compiler_params=pltpu.CompilerParams(vmem_limit_bytes=4 * 2**20),
        name="deliver",
    )(input_grad, up_grad, down_grad)


def solution(mesh):
    placed = (
        P(("fs", "tp"), None),
        P("fs", "tp"),
        P(("fs", "tp"), None),
        P("fs", "tp"),
        P("tp", "fs"),
    )
    return jax.shard_map(
        local,
        mesh=mesh,
        in_specs=placed,
        out_specs=(P(("fs", "tp"), None), P("fs", "tp"), P("tp", "fs")),
        check_vma=False,
    )
```

```python
import math

import jax
import jax.numpy as jnp
from jax import lax
from jax.experimental import pallas as pl
from jax.experimental.pallas import tpu as pltpu
from jax.sharding import PartitionSpec as P

MESH = pl.DeviceIdType.MESH
F32 = jnp.float32
BF16 = jnp.bfloat16
SENDS, RECVS = 8, 38


def rem4(value):
    return lax.rem(value, 4)


def nt(a, b):
    return lax.dot_general(a, b, (((1,), (1,)), ((), ())), preferred_element_type=F32)


def nn(a, b):
    return jnp.dot(a, b, preferred_element_type=F32)


def size_of(ref):
    return 2 * math.prod(ref.shape)


class Wires:
    def __init__(self, send_sem, recv_sem, partner, filler):
        self.send_sem, self.recv_sem, self.partner = send_sem, recv_sem, partner
        self.filler = filler
        self.groups, self.keys, self.bytes = {}, {}, {}

    def group(self, name):
        return self.groups.setdefault(name, len(self.groups))

    def key(self, name):
        return self.keys.setdefault(name, len(self.keys))

    def copy(self, g, k, src, dst, device):
        return pltpu.make_async_remote_copy(
            src_ref=src,
            dst_ref=dst,
            send_sem=self.send_sem.at[g],
            recv_sem=self.recv_sem.at[k],
            device_id=device,
            device_id_type=MESH,
        )

    def send(self, group, key, src, dst, device):
        self.copy(self.group(group), self.key(key), src, dst, device).start()
        self.bytes[group] = self.bytes.get(group, 0) + size_of(src)

    def recv(self, key, size):
        ref = self.filler(size)
        self.copy(0, self.key(key), ref, ref, self.partner).wait_recv()

    def drain(self, group):
        ref = self.filler(self.bytes[group])
        self.copy(self.group(group), 0, ref, ref, self.partner).wait_send()


class Gather:
    share = 1

    def __init__(self, wires, group, tag, pos, right, left, piece):
        self.w, self.group, self.tag, self.pos = wires, group, tag, pos
        self.right, self.left, self.piece = right, left, piece
        self.size = size_of(piece(pos, 0))

    def wait(self, name, pieces):
        if self.share:
            self.w.recv((self.tag, name), self.share * pieces * self.size)

    def at(self, hop, p):
        return self.piece(rem4(self.pos + hop), p)

    def put(self, name, hop, p, device):
        ref = self.at(hop, p)
        self.w.send(self.group, (self.tag, name), ref, ref, device)

    def own(self):
        self.put("first", 0, 0, self.right)
        self.put("first", 0, 1, self.left)
        self.put("near", 0, 1, self.right)
        self.put("near", 0, 0, self.left)

    def forward(self):
        self.wait("first", 2)
        self.put("far", 3, 0, self.right)
        self.put("far", 1, 1, self.left)

    def near(self):
        self.wait("near", 2)

    def far(self):
        self.wait("far", 2)


class QuarterGather(Gather):
    def __init__(self, wires, group, tag, pos, right, left, piece, quarter):
        super().__init__(wires, group, tag, pos, right, left, piece)
        self.quarter = quarter

    def give(self, turn, *members):
        name = (self.tag, "near" if turn else "first")
        for h in members:
            for device, p in ((self.right, turn), (self.left, 1 - turn)):
                ref = self.quarter(self.pos, p, h)
                self.w.send(self.group, name, ref, ref, device)


class Scatter:
    share = 1
    near_name = "last"

    def __init__(self, wires, group, tag, pos, right, left, piece, landing):
        self.w, self.group, self.tag, self.pos = wires, group, tag, pos
        self.right, self.left = right, left
        self.piece, self.landing = piece, landing
        self.size = size_of(piece(pos, 0))

    def wait(self, name, quarters):
        if self.share:
            self.w.recv((self.tag, name), self.share * quarters * self.size // 4)

    def at(self, hop, p):
        return self.piece(rem4(self.pos + hop), p)

    def put(self, name, side, m, hop, p):
        self.w.send(
            self.group,
            (self.tag, name),
            self.at(hop, p),
            self.landing(side, m),
            self.right if side == 0 else self.left,
        )

    def far(self):
        self.put("first", 0, 0, 2, 0)
        self.put("first", 1, 0, 2, 1)

    def to_right(self):
        self.put(self.near_name, 0, 1, 1, 1)

    def to_left(self):
        self.put(self.near_name, 1, 1, 3, 0)

    def add_first(self):
        self.wait("first", 8)
        for side, hop, p in ((0, 1, 0), (1, 3, 1)):
            came, mine = self.landing(side, 0), self.at(hop, p)
            mine[...] = (mine[...].astype(F32) + came[...].astype(F32)).astype(BF16)

    def middle(self):
        self.add_first()
        self.put("last", 0, 2, 1, 0)
        self.put("last", 1, 2, 3, 1)

    def finish(self, store=None):
        self.wait("last", 16)
        for p, near, far in ((1, 0, 1), (0, 1, 0)):
            first, second = self.landing(near, 1), self.landing(far, 2)
            mine = self.at(0, p)
            total = mine[...].astype(F32) + first[...].astype(F32) + second[...].astype(F32)
            if store is None:
                mine[...] = total.astype(BF16)
            else:
                store(p, total)


class StagedScatter(Scatter):
    near_name = "near"

    def begin(self, store):
        self.wait("near", 8)
        for p, side in ((1, 0), (0, 1)):
            store(p, self.at(0, p)[...].astype(F32) + self.landing(side, 1)[...].astype(F32))

    def end(self, add):
        self.wait("last", 8)
        for p, side in ((1, 1), (0, 0)):
            add(p, self.landing(side, 2)[...])


class QuarterScatter(Scatter):
    def __init__(self, wires, group, tag, pos, right, left, piece, landing, quarter, landed):
        super().__init__(wires, group, tag, pos, right, left, piece, landing)
        self.quarter, self.landed = quarter, landed

    def give(self, *members):
        for h in members:
            for side, hop, p in ((0, 1, 0), (1, 3, 1)):
                self.w.send(
                    self.group,
                    (self.tag, h),
                    self.quarter(rem4(self.pos + hop), p, h),
                    self.landed(side, 2, h),
                    self.right if side == 0 else self.left,
                )

    def near(self, *members):
        for h in members:
            for side, hop, p in ((0, 1, 1), (1, 3, 0)):
                self.w.send(
                    self.group,
                    (self.tag, h),
                    self.quarter(rem4(self.pos + hop), p, h),
                    self.landed(side, 1, h),
                    self.right if side == 0 else self.left,
                )

    def settle(self, h):
        self.wait(h, 4)
        for p, near, far in ((1, 0, 1), (0, 1, 0)):
            first, second = self.landed(near, 1, h), self.landed(far, 2, h)
            mine = self.quarter(self.pos, p, h)
            total = mine[...].astype(F32) + first[...].astype(F32) + second[...].astype(F32)
            mine[...] = total.astype(BF16)


def paired(first, second):
    second.tag, first.share, second.share = first.tag, 2, 0
    return first, second


def kernel(
    ni_hbm, pa_hbm, og_hbm, uw_hbm, dw_hbm,
    ig, ug, dg,
    ni, og, wd, wu, pg, ht, pgt, part, gd,
    cross, xland, zland_d, yland_d, yone_d, zone_d,
    zland_u, yland_u, yone_u, zone_u,
    send_sem, recv_sem, local_sem,
):
    fs, tp = lax.axis_index("fs"), lax.axis_index("tp")
    z, y, x, c = fs // 4, rem4(fs), tp // 2, lax.rem(tp, 2)
    x_right = {"fs": fs, "tp": rem4(x + 1) * 2 + c}
    x_left = {"fs": fs, "tp": rem4(x + 3) * 2 + c}
    y_right = {"fs": z * 4 + rem4(y + 1), "tp": tp}
    y_left = {"fs": z * 4 + rem4(y + 3), "tp": tp}
    z_right = {"fs": rem4(z + 1) * 4 + y, "tp": tp}
    z_left = {"fs": rem4(z + 3) * 4 + y, "tp": tp}
    partner = {"fs": fs, "tp": x * 2 + 1 - c}

    rows = og_hbm.shape[0]
    half = rows // 2
    ff, cols = dw_hbm.shape
    wide = 4 * cols
    quarter = ff // 4
    urows = uw_hbm.shape[0]
    tokens = pg.shape[0]

    line = 2 * og.shape[1]
    w = Wires(send_sem, recv_sem, partner, lambda size: og.at[pl.ds(0, size // line), :])

    def token_rows(ref, block):
        return ref.at[pl.ds(pl.multiple_of(block * rows, rows), rows), :]

    def lanes(i):
        return pl.ds(pl.multiple_of(i * cols, cols), cols)

    mine = [
        (dw_hbm, wd.at[z, :, lanes(y)]),
        (og_hbm, token_rows(og, tp)),
        (uw_hbm, wu.at[z, y]),
        (pa_hbm, pg),
        (ni_hbm, token_rows(ni, tp)),
    ]
    local = [
        pltpu.make_async_copy(src, dst, local_sem.at[i])
        for i, (src, dst) in enumerate(mine)
    ]
    barrier = pltpu.get_barrier_semaphore()
    for device in (x_right, x_left, y_right, y_left, z_right, z_left, partner):
        pl.semaphore_signal(barrier, inc=1, device_id=device, device_id_type=MESH)
    for copy in local:
        copy.start()
    pl.semaphore_wait(barrier, 7)

    def wd_rows(p):
        return pl.ds(p * quarter, quarter)

    def wu_rows(p):
        return pl.ds(p * (urows // 4), urows // 4)

    def weight_rings(tag, one, z_group, y_group):
        return (
            (
                Gather(w, tag, tag + "a1", y, y_right, y_left, lambda i, p: one(z, i, p)),
                Gather(w, tag, tag + "b1", z, z_right, z_left, lambda i, p: one(i, y, 2 + p)),
            ),
            (
                Gather(w, tag, tag + "a2", z, z_right, z_left, lambda i, p: z_group(i, p)),
                Gather(w, tag, tag + "b2", y, y_right, y_left, lambda i, p: y_group(i, 2 + p)),
            ),
        )

    wd1, _ = weight_rings(
        "d",
        lambda zi, yi, p: wd.at[zi, wd_rows(p), lanes(yi)],
        lambda zi, p: wd.at[zi, wd_rows(p), :],
        lambda yi, p: wd.at[:, wd_rows(p), lanes(yi)],
    )
    wd2 = (
        QuarterGather(
            w, "d", "da2", z, z_right, z_left,
            lambda i, p: wd.at[i, wd_rows(p), :],
            lambda i, p, h: wd.at[i, wd_rows(p), lanes(rem4(y + h))],
        ),
        QuarterGather(
            w, "d", "db2", y, y_right, y_left,
            lambda i, p: wd.at[:, wd_rows(2 + p), lanes(i)],
            lambda i, p, h: wd.at[rem4(z + h), wd_rows(2 + p), lanes(i)],
        ),
    )
    wu1, wu2 = weight_rings(
        "u",
        lambda zi, yi, p: wu.at[zi, yi, wu_rows(p), :],
        lambda zi, p: wu.at[zi, :, wu_rows(p), :],
        lambda yi, p: wu.at[:, yi, wu_rows(p), :],
    )

    for pair in (wd1, wd2, wu1, wu2):
        paired(*pair)

    def token_piece(ref, core):
        def piece(i, p):
            start = pl.multiple_of((i * 2 + core) * rows + p * half, half)
            return ref.at[pl.ds(start, half), :]

        return piece

    rings = {
        "o": Gather(w, "o", "o", x, x_right, x_left, token_piece(og, c)),
        "n": Gather(w, "n", "n", x, x_right, x_left, token_piece(ni, c)),
    }

    def hand(tag, *pieces):
        for hop, p in pieces:
            ref = rings[tag].at(hop, p)
            w.send(tag, (tag, "cross"), ref, ref, partner)

    def handed(tag):
        w.recv((tag, "cross"), 8 * rings[tag].size)

    def token_own(tag):
        rings[tag].own()
        hand(tag, (0, 0), (0, 1))

    def token_forward(tag):
        rings[tag].forward()
        hand(tag, (3, 0), (1, 1))

    def token_near(tag):
        rings[tag].near()
        hand(tag, (3, 1), (1, 0))

    def token_far(tag):
        rings[tag].far()
        hand(tag, (2, 0), (2, 1))

    def each(pair, step):
        for ring in pair:
            getattr(ring, step)()

    def hidden(count, first):
        def body(j, carry):
            at = pl.multiple_of(j * 128, 128)
            active = jnp.maximum(pg[pl.ds(at, 128), :].astype(F32), 0.0)
            ht[:, pl.ds(at, 128)] = (active * active).astype(BF16).T
            return carry

        lax.fori_loop(first, first + count, body, 0)

    def give(pair, *what):
        for ring in pair:
            ring.give(*what)

    local[0].wait()
    each(wd1, "own")
    local[1].wait()
    token_own("o")
    local[2].wait()
    each(wu1, "own")
    give(wd2, 0, 0)
    give(wd2, 1, 0)
    local[3].wait()
    hidden(6, 0)
    each(wd1, "forward")
    each(wu1, "forward")
    hidden(6, 6)
    each(wd1, "near")
    give(wd2, 0, 1, 3)
    token_forward("o")
    each(wd1, "far")
    give(wd2, 0, 2)
    give(wd2, 1, 1, 3, 2)
    local[4].wait()
    token_own("n")
    each(wu1, "near")
    each(wu1, "far")
    each(wd2, "forward")
    each(wu2, "own")
    token_near("o")
    token_far("o")
    each(wd2, "near")
    each(wd2, "far")
    handed("o")

    block = 256

    def pre_grad(i, carry):
        at = pl.ds(pl.multiple_of(i * block, block), block)
        for n in range(2):
            units = pl.ds(n * ff // 2, ff // 2)
            weight = jnp.concatenate([wd[k, units, :] for k in range(4)], axis=1)
            grad = nt(og[at, :], weight)
            active = jnp.maximum(pg[at, units].astype(F32), 0.0)
            value = (2.0 * active * grad).astype(BF16)
            pg[at, units] = value
            pgt[units, at] = value.T

        @pl.when(i == 2)
        def _():
            each(wu2, "forward")

        @pl.when(i == 5)
        def _():
            token_forward("n")

        return carry

    lax.fori_loop(0, tokens // block, pre_grad, 0)

    def grad_rings(tag, grad, zland, yland, yone, zone, kind):
        return (
            (
                Scatter(
                    w, tag, tag + "a1", z, z_right, z_left,
                    lambda i, p: grad.at[i, wd_rows(p), :],
                    lambda side, m: zland.at[side, m],
                ),
                Scatter(
                    w, tag, tag + "b1", y, y_right, y_left,
                    lambda i, p: grad.at[:, wd_rows(2 + p), lanes(i)],
                    lambda side, m: yland.at[side, m],
                ),
            ),
            (
                kind(
                    w, tag, tag + "a2", y, y_right, y_left,
                    lambda i, p: grad.at[z, wd_rows(p), lanes(i)],
                    lambda side, m: yone.at[side, m],
                ),
                kind(
                    w, tag, tag + "b2", z, z_right, z_left,
                    lambda i, p: grad.at[i, wd_rows(2 + p), lanes(y)],
                    lambda side, m: zone.at[side, m],
                ),
            ),
        )

    gd1, gd2 = grad_rings("D", gd, zland_d, yland_d, yone_d, zone_d, Scatter)
    gu = wd
    _, gu2 = grad_rings("U", gu, zland_u, yland_u, yone_u, zone_u, StagedScatter)
    gu1 = (
        QuarterScatter(
            w, "U", "Ua1", z, z_right, z_left,
            lambda i, p: gu.at[i, wd_rows(p), :],
            lambda side, m: zland_u.at[side, m],
            lambda i, p, h: gu.at[i, wd_rows(p), lanes(rem4(y + h))],
            lambda side, m, h: zland_u.at[side, m, :, lanes(rem4(y + h))],
        ),
        QuarterScatter(
            w, "U", "Ub1", y, y_right, y_left,
            lambda i, p: gu.at[:, wd_rows(2 + p), lanes(i)],
            lambda side, m: yland_u.at[side, m],
            lambda i, p, h: gu.at[rem4(z + h), wd_rows(2 + p), lanes(i)],
            lambda side, m, h: yland_u.at[side, m, rem4(z + h)],
        ),
    )
    for pair in (gd1, gd2, gu1, gu2):
        paired(*pair)
    upper = ff // 2

    def hop_of(k):
        return jnp.where(k == 0, 2, jnp.where(k == 1, 1, jnp.where(k == 2, 3, 0)))

    def weight_grad(left, right, grad, first, steps, extra):
        def body(k, carry):
            zi, yi = rem4(z + hop_of(k)), rem4(y + hop_of(k))
            strip = right[:, pl.ds(pl.multiple_of(zi * wide, wide), wide)]
            grad[zi, :upper, :] = nn(left[:upper, :], strip).astype(BF16)
            strip = jnp.concatenate(
                [right[:, pl.ds(pl.multiple_of(g * wide + yi * cols, cols), cols)] for g in range(4)],
                axis=1,
            )
            value = nn(left[upper:, :], strip).astype(BF16)
            for g in range(4):
                grad[g, upper:, lanes(yi)] = value[:, g * cols : (g + 1) * cols]

            if extra:
                extra(k)
            for turn, step in enumerate(steps):

                @pl.when(k == turn)
                def _(step=step):
                    each(first, step)

            return carry

        lax.fori_loop(0, 4, body, 0)

    weight_grad(ht, og, gd, gd1, ("far", "to_right", "to_left"), None)

    each(wu2, "near")
    each(wu2, "far")

    def share(block):
        return part.at[block]

    xs = Scatter(
        w, "x", "x", x, x_right, x_left,
        lambda i, p: part.at[i * 2 + c, pl.ds(p * half, half), :],
        lambda side, m: xland.at[side, m],
    )
    cross_base = [w.key(("c", k)) for k in range(4)][0]
    cross_group = w.group("c")
    w.bytes["c"] = size_of(cross)

    def product(xi):
        at = pl.ds(pl.multiple_of(xi * 2 * rows, 2 * rows), 2 * rows)
        for g in range(4):
            value = nt(pg[at, :], wu[g].reshape(4 * urows, ff)).astype(BF16)
            out = pl.ds(g * 4 * urows, 4 * urows)
            part[xi * 2, :, out] = value[:rows]
            part[xi * 2 + 1, :, out] = value[rows:]

    def send_cross(k):
        block = part.at[rem4(x + hop_of(k)) * 2 + 1 - c]
        w.copy(cross_group, cross_base + k, block, cross.at[k], partner).start()

    def add_cross(k):
        index = rem4(x + hop_of(k)) * 2 + c
        w.copy(cross_group, cross_base + k, cross.at[k], cross.at[k], partner).wait_recv()
        total = part[index].astype(F32) + cross[k].astype(F32)
        part[index] = total.astype(BF16)

    def input_grad(k, carry):
        xi = rem4(x + hop_of(k))
        product(xi)

        @pl.when(k == 2)
        def _():
            token_far("n")

        send_cross(k)

        @pl.when(k == 0)
        def _():
            token_near("n")

        @pl.when(k == 1)
        def _():
            each(gd1, "middle")
            add_cross(0)
            xs.far()

        @pl.when(k == 2)
        def _():
            add_cross(1)
            xs.to_right()

        return carry

    lax.fori_loop(0, 3, input_grad, 0)
    handed("n")
    w.drain("d")

    def near(*members):
        for ring in gu1:
            ring.near(*members)

    def while_up(k):
        @pl.when(k == 0)
        def _():
            add_cross(2)
            xs.to_left()

        @pl.when(k == 1)
        def _():
            each(gd1, "finish")
            each(gd2, "far")
            each(gd2, "to_right")
            each(gd2, "to_left")

        @pl.when(k == 2)
        def _():
            near(2)
            xs.middle()

    weight_grad(pgt, ni, gu, gu1, ("far",), while_up)

    def settle(h):
        for ring in gu1:
            ring.settle(h)

    near(1)
    each(gu1, "add_first")
    give(gu1, 2, 1)
    near(3)
    give(gu1, 3)
    product(x)
    send_cross(3)
    each(gd2, "middle")
    settle(2)
    each(gu2, "far")
    near(0)
    give(gu1, 0)
    settle(1)
    each(gu2, "to_right")
    settle(3)
    each(gu2, "to_left")
    add_cross(3)
    each(gu2, "middle")
    settle(0)
    for i, ring in enumerate(gu2):

        def store_up(p, total, i=i):
            ug[:, wd_rows(2 * i + p)] = total.T

        ring.begin(store_up)

    def store_rows(p, total):
        ig[pl.ds(p * half, half), :] = total.astype(BF16)

    xs.finish(store_rows)
    for i, ring in enumerate(gd2):

        def store_down(p, total, i=i):
            dg[wd_rows(2 * i + p), :] = total

        ring.finish(store_down)
    for i, ring in enumerate(gu2):

        def add_up(p, came, i=i):
            at = wd_rows(2 * i + p)
            ug[:, at] = ug[:, at] + came.T.astype(F32)

        ring.end(add_up)
    for group in ("u", "o", "n", "D", "U", "x", "c"):
        w.drain(group)


def deliver(*refs):
    sem = refs[-1]
    copies = [pltpu.make_async_copy(refs[i], refs[3 + i], sem.at[i]) for i in range(3)]
    for copy in copies:
        copy.start()
    for copy in copies:
        copy.wait()


def local(normed_input, pre_act, out_grad, up_weight, down_weight):
    rows, d = out_grad.shape
    tokens, ff = pre_act.shape
    cols = down_weight.shape[1]
    quarter = ff // 4
    half = rows // 2
    grads = [
        pltpu.VMEM((2, 3, quarter, 4 * cols), BF16),
        pltpu.VMEM((2, 3, 4, quarter, cols), BF16),
        pltpu.VMEM((2, 3, quarter, cols), BF16),
        pltpu.VMEM((2, 3, quarter, cols), BF16),
    ]
    input_grad, up_grad, down_grad = pl.pallas_call(
        kernel,
        out_shape=(
            pltpu.VMEM((rows, d), BF16),
            pltpu.VMEM((cols, ff), F32),
            pltpu.VMEM((ff, cols), F32),
        ),
        in_specs=[pl.BlockSpec(memory_space=pltpu.HBM)] * 5,
        out_specs=(pl.BlockSpec(memory_space=pltpu.VMEM),) * 3,
        scratch_shapes=[
            pltpu.VMEM((tokens, d), BF16),
            pltpu.VMEM((tokens, d), BF16),
            pltpu.VMEM((4, ff, 4 * cols), BF16),
            pltpu.VMEM((4, 4, d // 16, ff), BF16),
            pltpu.VMEM((tokens, ff), BF16),
            pltpu.VMEM((ff, tokens), BF16),
            pltpu.VMEM((ff, tokens), BF16),
            pltpu.VMEM((8, rows, d), BF16),
            pltpu.VMEM((4, ff, 4 * cols), BF16),
            pltpu.VMEM((4, rows, d), BF16),
            pltpu.VMEM((2, 3, half, d), BF16),
            *grads,
            *grads,
            pltpu.SemaphoreType.DMA((SENDS,)),
            pltpu.SemaphoreType.DMA((RECVS,)),
            pltpu.SemaphoreType.DMA((5,)),
        ],
        compiler_params=pltpu.CompilerParams(
            collective_id=0,
            has_side_effects=True,
            vmem_limit_bytes=62800000,
        ),
        name="ffn_backward",
    )(normed_input, pre_act, out_grad, up_weight, down_weight)
    return pl.pallas_call(
        deliver,
        out_shape=(
            jax.ShapeDtypeStruct((rows, d), BF16),
            jax.ShapeDtypeStruct((cols, ff), F32),
            jax.ShapeDtypeStruct((ff, cols), F32),
        ),
        in_specs=[pl.BlockSpec(memory_space=pl.ANY)] * 3,
        out_specs=(pl.BlockSpec(memory_space=pl.ANY),) * 3,
        scratch_shapes=[pltpu.SemaphoreType.DMA((3,))],
        compiler_params=pltpu.CompilerParams(vmem_limit_bytes=4 * 2**20),
        name="deliver",
    )(input_grad, up_grad, down_grad)


def solution(mesh):
    placed = (
        P(("fs", "tp"), None),
        P("fs", "tp"),
        P(("fs", "tp"), None),
        P("fs", "tp"),
        P("tp", "fs"),
    )
    return jax.shard_map(
        local,
        mesh=mesh,
        in_specs=placed,
        out_specs=(P(("fs", "tp"), None), P("fs", "tp"), P("tp", "fs")),
        check_vma=False,
    )
```

```python
import math

import jax
import jax.numpy as jnp
from jax import lax
from jax.experimental import pallas as pl
from jax.experimental.pallas import tpu as pltpu
from jax.sharding import PartitionSpec as P

MESH = pl.DeviceIdType.MESH
F32 = jnp.float32
BF16 = jnp.bfloat16
SENDS, RECVS = 8, 38


def rem4(value):
    return lax.rem(value, 4)


def nt(a, b):
    return lax.dot_general(a, b, (((1,), (1,)), ((), ())), preferred_element_type=F32)


def nn(a, b):
    return jnp.dot(a, b, preferred_element_type=F32)


def size_of(ref):
    return 2 * math.prod(ref.shape)


class Wires:
    def __init__(self, send_sem, recv_sem, partner, filler):
        self.send_sem, self.recv_sem, self.partner = send_sem, recv_sem, partner
        self.filler = filler
        self.groups, self.keys, self.bytes = {}, {}, {}

    def group(self, name):
        return self.groups.setdefault(name, len(self.groups))

    def key(self, name):
        return self.keys.setdefault(name, len(self.keys))

    def copy(self, g, k, src, dst, device):
        return pltpu.make_async_remote_copy(
            src_ref=src,
            dst_ref=dst,
            send_sem=self.send_sem.at[g],
            recv_sem=self.recv_sem.at[k],
            device_id=device,
            device_id_type=MESH,
        )

    def send(self, group, key, src, dst, device):
        self.copy(self.group(group), self.key(key), src, dst, device).start()
        self.bytes[group] = self.bytes.get(group, 0) + size_of(src)

    def recv(self, key, size):
        ref = self.filler(size)
        self.copy(0, self.key(key), ref, ref, self.partner).wait_recv()

    def drain(self, group):
        ref = self.filler(self.bytes[group])
        self.copy(self.group(group), 0, ref, ref, self.partner).wait_send()


class Gather:
    share = 1

    def __init__(self, wires, group, tag, pos, right, left, piece):
        self.w, self.group, self.tag, self.pos = wires, group, tag, pos
        self.right, self.left, self.piece = right, left, piece
        self.size = size_of(piece(pos, 0))

    def wait(self, name, pieces):
        if self.share:
            self.w.recv((self.tag, name), self.share * pieces * self.size)

    def at(self, hop, p):
        return self.piece(rem4(self.pos + hop), p)

    def put(self, name, hop, p, device):
        ref = self.at(hop, p)
        self.w.send(self.group, (self.tag, name), ref, ref, device)

    def own(self):
        self.put("first", 0, 0, self.right)
        self.put("first", 0, 1, self.left)
        self.put("near", 0, 1, self.right)
        self.put("near", 0, 0, self.left)

    def forward(self):
        self.wait("first", 2)
        self.put("far", 3, 0, self.right)
        self.put("far", 1, 1, self.left)

    def near(self):
        self.wait("near", 2)

    def far(self):
        self.wait("far", 2)


class QuarterGather(Gather):
    def __init__(self, wires, group, tag, pos, right, left, piece, quarter):
        super().__init__(wires, group, tag, pos, right, left, piece)
        self.quarter = quarter

    def give(self, turn, *members):
        name = (self.tag, "near" if turn else "first")
        for h in members:
            for device, p in ((self.right, turn), (self.left, 1 - turn)):
                ref = self.quarter(self.pos, p, h)
                self.w.send(self.group, name, ref, ref, device)


class Scatter:
    share = 1

    def __init__(self, wires, group, tag, pos, right, left, piece, landing):
        self.w, self.group, self.tag, self.pos = wires, group, tag, pos
        self.right, self.left = right, left
        self.piece, self.landing = piece, landing
        self.size = size_of(piece(pos, 0))

    def wait(self, name, quarters):
        if self.share:
            self.w.recv((self.tag, name), self.share * quarters * self.size // 4)

    def at(self, hop, p):
        return self.piece(rem4(self.pos + hop), p)

    def put(self, name, side, m, hop, p):
        self.w.send(
            self.group,
            (self.tag, name),
            self.at(hop, p),
            self.landing(side, m),
            self.right if side == 0 else self.left,
        )

    def far(self):
        self.put("first", 0, 0, 2, 0)
        self.put("first", 1, 0, 2, 1)

    def to_right(self):
        self.put("last", 0, 1, 1, 1)

    def to_left(self):
        self.put("last", 1, 1, 3, 0)

    def add_first(self):
        self.wait("first", 8)
        for side, hop, p in ((0, 1, 0), (1, 3, 1)):
            came, mine = self.landing(side, 0), self.at(hop, p)
            mine[...] = (mine[...].astype(F32) + came[...].astype(F32)).astype(BF16)

    def middle(self):
        self.add_first()
        self.put("last", 0, 2, 1, 0)
        self.put("last", 1, 2, 3, 1)

    def finish(self, store=None):
        self.wait("last", 16)
        for p, near, far in ((1, 0, 1), (0, 1, 0)):
            first, second = self.landing(near, 1), self.landing(far, 2)
            mine = self.at(0, p)
            total = mine[...].astype(F32) + first[...].astype(F32) + second[...].astype(F32)
            if store is None:
                mine[...] = total.astype(BF16)
            else:
                store(p, total)


class QuarterScatter(Scatter):
    def __init__(self, wires, group, tag, pos, right, left, piece, landing, quarter, landed):
        super().__init__(wires, group, tag, pos, right, left, piece, landing)
        self.quarter, self.landed = quarter, landed

    def give(self, *members):
        for h in members:
            for side, hop, p in ((0, 1, 0), (1, 3, 1)):
                self.w.send(
                    self.group,
                    (self.tag, h),
                    self.quarter(rem4(self.pos + hop), p, h),
                    self.landed(side, 2, h),
                    self.right if side == 0 else self.left,
                )

    def near(self, *members):
        for h in members:
            for side, hop, p in ((0, 1, 1), (1, 3, 0)):
                self.w.send(
                    self.group,
                    (self.tag, h),
                    self.quarter(rem4(self.pos + hop), p, h),
                    self.landed(side, 1, h),
                    self.right if side == 0 else self.left,
                )

    def settle(self, h):
        self.wait(h, 4)
        for p, near, far in ((1, 0, 1), (0, 1, 0)):
            first, second = self.landed(near, 1, h), self.landed(far, 2, h)
            mine = self.quarter(self.pos, p, h)
            total = mine[...].astype(F32) + first[...].astype(F32) + second[...].astype(F32)
            mine[...] = total.astype(BF16)


def paired(first, second):
    second.tag, first.share, second.share = first.tag, 2, 0
    return first, second


def kernel(
    ni_hbm, pa_hbm, og_hbm, uw_hbm, dw_hbm,
    ig, ug, dg,
    ni, og, wd, wu, pg, ht, pgt, part, gd,
    cross, xland, zland_d, yland_d, yone_d, zone_d,
    zland_u, yland_u, yone_u, zone_u,
    send_sem, recv_sem, local_sem,
):
    fs, tp = lax.axis_index("fs"), lax.axis_index("tp")
    z, y, x, c = fs // 4, rem4(fs), tp // 2, lax.rem(tp, 2)
    x_right = {"fs": fs, "tp": rem4(x + 1) * 2 + c}
    x_left = {"fs": fs, "tp": rem4(x + 3) * 2 + c}
    y_right = {"fs": z * 4 + rem4(y + 1), "tp": tp}
    y_left = {"fs": z * 4 + rem4(y + 3), "tp": tp}
    z_right = {"fs": rem4(z + 1) * 4 + y, "tp": tp}
    z_left = {"fs": rem4(z + 3) * 4 + y, "tp": tp}
    partner = {"fs": fs, "tp": x * 2 + 1 - c}

    rows = og_hbm.shape[0]
    half = rows // 2
    ff, cols = dw_hbm.shape
    wide = 4 * cols
    quarter = ff // 4
    urows = uw_hbm.shape[0]
    tokens = pg.shape[0]

    line = 2 * og.shape[1]
    w = Wires(send_sem, recv_sem, partner, lambda size: og.at[pl.ds(0, size // line), :])

    def token_rows(ref, block):
        return ref.at[pl.ds(pl.multiple_of(block * rows, rows), rows), :]

    def lanes(i):
        return pl.ds(pl.multiple_of(i * cols, cols), cols)

    mine = [
        (dw_hbm, wd.at[z, :, lanes(y)]),
        (og_hbm, token_rows(og, tp)),
        (uw_hbm, wu.at[z, y]),
        (pa_hbm, pg),
        (ni_hbm, token_rows(ni, tp)),
    ]
    local = [
        pltpu.make_async_copy(src, dst, local_sem.at[i])
        for i, (src, dst) in enumerate(mine)
    ]
    barrier = pltpu.get_barrier_semaphore()
    for device in (x_right, x_left, y_right, y_left, z_right, z_left, partner):
        pl.semaphore_signal(barrier, inc=1, device_id=device, device_id_type=MESH)
    for copy in local:
        copy.start()
    pl.semaphore_wait(barrier, 7)

    def wd_rows(p):
        return pl.ds(p * quarter, quarter)

    def wu_rows(p):
        return pl.ds(p * (urows // 4), urows // 4)

    def weight_rings(tag, one, z_group, y_group):
        return (
            (
                Gather(w, tag, tag + "a1", y, y_right, y_left, lambda i, p: one(z, i, p)),
                Gather(w, tag, tag + "b1", z, z_right, z_left, lambda i, p: one(i, y, 2 + p)),
            ),
            (
                Gather(w, tag, tag + "a2", z, z_right, z_left, lambda i, p: z_group(i, p)),
                Gather(w, tag, tag + "b2", y, y_right, y_left, lambda i, p: y_group(i, 2 + p)),
            ),
        )

    wd1, _ = weight_rings(
        "d",
        lambda zi, yi, p: wd.at[zi, wd_rows(p), lanes(yi)],
        lambda zi, p: wd.at[zi, wd_rows(p), :],
        lambda yi, p: wd.at[:, wd_rows(p), lanes(yi)],
    )
    wd2 = (
        QuarterGather(
            w, "d", "da2", z, z_right, z_left,
            lambda i, p: wd.at[i, wd_rows(p), :],
            lambda i, p, h: wd.at[i, wd_rows(p), lanes(rem4(y + h))],
        ),
        QuarterGather(
            w, "d", "db2", y, y_right, y_left,
            lambda i, p: wd.at[:, wd_rows(2 + p), lanes(i)],
            lambda i, p, h: wd.at[rem4(z + h), wd_rows(2 + p), lanes(i)],
        ),
    )
    wu1, wu2 = weight_rings(
        "u",
        lambda zi, yi, p: wu.at[zi, yi, wu_rows(p), :],
        lambda zi, p: wu.at[zi, :, wu_rows(p), :],
        lambda yi, p: wu.at[:, yi, wu_rows(p), :],
    )

    for pair in (wd1, wd2, wu1, wu2):
        paired(*pair)

    def token_piece(ref, core):
        def piece(i, p):
            start = pl.multiple_of((i * 2 + core) * rows + p * half, half)
            return ref.at[pl.ds(start, half), :]

        return piece

    rings = {
        "o": Gather(w, "o", "o", x, x_right, x_left, token_piece(og, c)),
        "n": Gather(w, "n", "n", x, x_right, x_left, token_piece(ni, c)),
    }

    def hand(tag, *pieces):
        for hop, p in pieces:
            ref = rings[tag].at(hop, p)
            w.send(tag, (tag, "cross"), ref, ref, partner)

    def handed(tag):
        w.recv((tag, "cross"), 8 * rings[tag].size)

    def token_own(tag):
        rings[tag].own()
        hand(tag, (0, 0), (0, 1))

    def token_forward(tag):
        rings[tag].forward()
        hand(tag, (3, 0), (1, 1))

    def token_near(tag):
        rings[tag].near()
        hand(tag, (3, 1), (1, 0))

    def token_far(tag):
        rings[tag].far()
        hand(tag, (2, 0), (2, 1))

    def each(pair, step):
        for ring in pair:
            getattr(ring, step)()

    def hidden(count, first):
        def body(j, carry):
            at = pl.multiple_of(j * 128, 128)
            active = jnp.maximum(pg[pl.ds(at, 128), :].astype(F32), 0.0)
            ht[:, pl.ds(at, 128)] = (active * active).astype(BF16).T
            return carry

        lax.fori_loop(first, first + count, body, 0)

    def give(pair, *what):
        for ring in pair:
            ring.give(*what)

    local[0].wait()
    each(wd1, "own")
    local[1].wait()
    token_own("o")
    local[2].wait()
    each(wu1, "own")
    give(wd2, 0, 0)
    give(wd2, 1, 0)
    local[3].wait()
    hidden(6, 0)
    each(wd1, "forward")
    each(wu1, "forward")
    hidden(6, 6)
    each(wd1, "near")
    give(wd2, 0, 1, 3)
    token_forward("o")
    each(wd1, "far")
    give(wd2, 0, 2)
    give(wd2, 1, 1, 3, 2)
    local[4].wait()
    token_own("n")
    each(wu1, "near")
    each(wu1, "far")
    each(wd2, "forward")
    each(wu2, "own")
    token_near("o")
    token_far("o")
    each(wd2, "near")
    each(wd2, "far")
    handed("o")

    block = 256

    def pre_grad(i, carry):
        at = pl.ds(pl.multiple_of(i * block, block), block)
        for n in range(2):
            units = pl.ds(n * ff // 2, ff // 2)
            weight = jnp.concatenate([wd[k, units, :] for k in range(4)], axis=1)
            grad = nt(og[at, :], weight)
            active = jnp.maximum(pg[at, units].astype(F32), 0.0)
            value = (2.0 * active * grad).astype(BF16)
            pg[at, units] = value
            pgt[units, at] = value.T

        @pl.when(i == 2)
        def _():
            each(wu2, "forward")

        @pl.when(i == 5)
        def _():
            token_forward("n")

        return carry

    lax.fori_loop(0, tokens // block, pre_grad, 0)

    def grad_rings(tag, grad, zland, yland, yone, zone):
        return (
            (
                Scatter(
                    w, tag, tag + "a1", z, z_right, z_left,
                    lambda i, p: grad.at[i, wd_rows(p), :],
                    lambda side, m: zland.at[side, m],
                ),
                Scatter(
                    w, tag, tag + "b1", y, y_right, y_left,
                    lambda i, p: grad.at[:, wd_rows(2 + p), lanes(i)],
                    lambda side, m: yland.at[side, m],
                ),
            ),
            (
                Scatter(
                    w, tag, tag + "a2", y, y_right, y_left,
                    lambda i, p: grad.at[z, wd_rows(p), lanes(i)],
                    lambda side, m: yone.at[side, m],
                ),
                Scatter(
                    w, tag, tag + "b2", z, z_right, z_left,
                    lambda i, p: grad.at[i, wd_rows(2 + p), lanes(y)],
                    lambda side, m: zone.at[side, m],
                ),
            ),
        )

    gd1, gd2 = grad_rings("D", gd, zland_d, yland_d, yone_d, zone_d)
    gu = wd
    _, gu2 = grad_rings("U", gu, zland_u, yland_u, yone_u, zone_u)
    gu1 = (
        QuarterScatter(
            w, "U", "Ua1", z, z_right, z_left,
            lambda i, p: gu.at[i, wd_rows(p), :],
            lambda side, m: zland_u.at[side, m],
            lambda i, p, h: gu.at[i, wd_rows(p), lanes(rem4(y + h))],
            lambda side, m, h: zland_u.at[side, m, :, lanes(rem4(y + h))],
        ),
        QuarterScatter(
            w, "U", "Ub1", y, y_right, y_left,
            lambda i, p: gu.at[:, wd_rows(2 + p), lanes(i)],
            lambda side, m: yland_u.at[side, m],
            lambda i, p, h: gu.at[rem4(z + h), wd_rows(2 + p), lanes(i)],
            lambda side, m, h: yland_u.at[side, m, rem4(z + h)],
        ),
    )
    for pair in (gd1, gd2, gu1, gu2):
        paired(*pair)
    upper = ff // 2

    def hop_of(k):
        return jnp.where(k == 0, 2, jnp.where(k == 1, 1, jnp.where(k == 2, 3, 0)))

    def weight_grad(left, right, grad, first, steps, extra):
        def launch(k, ring):
            for turn, step in enumerate(steps):
                pl.when(k == turn)(getattr(ring, step))

        def body(k, carry):
            zi, yi = rem4(z + hop_of(k)), rem4(y + hop_of(k))
            strip = right[:, pl.ds(pl.multiple_of(zi * wide, wide), wide)]
            grad[zi, :upper, :] = nn(left[:upper, :], strip).astype(BF16)
            launch(k, first[0])
            strip = jnp.concatenate(
                [right[:, pl.ds(pl.multiple_of(g * wide + yi * cols, cols), cols)] for g in range(4)],
                axis=1,
            )
            value = nn(left[upper:, :], strip).astype(BF16)
            for g in range(4):
                grad[g, upper:, lanes(yi)] = value[:, g * cols : (g + 1) * cols]
            launch(k, first[1])
            if extra:
                extra(k)

            return carry

        lax.fori_loop(0, 4, body, 0)

    weight_grad(ht, og, gd, gd1, ("far", "to_right", "to_left"), None)

    each(wu2, "near")
    each(wu2, "far")

    def share(block):
        return part.at[block]

    xs = Scatter(
        w, "x", "x", x, x_right, x_left,
        lambda i, p: part.at[i * 2 + c, pl.ds(p * half, half), :],
        lambda side, m: xland.at[side, m],
    )
    cross_base = [w.key(("c", k)) for k in range(4)][0]
    cross_group = w.group("c")
    w.bytes["c"] = size_of(cross)

    def product(xi):
        at = pl.ds(pl.multiple_of(xi * 2 * rows, 2 * rows), 2 * rows)
        for g in range(4):
            value = nt(pg[at, :], wu[g].reshape(4 * urows, ff)).astype(BF16)
            out = pl.ds(g * 4 * urows, 4 * urows)
            part[xi * 2, :, out] = value[:rows]
            part[xi * 2 + 1, :, out] = value[rows:]

    def send_cross(k):
        block = part.at[rem4(x + hop_of(k)) * 2 + 1 - c]
        w.copy(cross_group, cross_base + k, block, cross.at[k], partner).start()

    def add_cross(k):
        index = rem4(x + hop_of(k)) * 2 + c
        w.copy(cross_group, cross_base + k, cross.at[k], cross.at[k], partner).wait_recv()
        total = part[index].astype(F32) + cross[k].astype(F32)
        part[index] = total.astype(BF16)

    def input_grad(k, carry):
        xi = rem4(x + hop_of(k))
        product(xi)

        @pl.when(k == 2)
        def _():
            token_far("n")

        send_cross(k)

        @pl.when(k == 0)
        def _():
            token_near("n")

        @pl.when(k == 1)
        def _():
            each(gd1, "middle")
            add_cross(0)
            xs.far()

        @pl.when(k == 2)
        def _():
            add_cross(1)
            xs.to_right()

        return carry

    lax.fori_loop(0, 3, input_grad, 0)
    handed("n")
    w.drain("d")

    def near(*members):
        for ring in gu1:
            ring.near(*members)

    def while_up(k):
        @pl.when(k == 0)
        def _():
            add_cross(2)
            xs.to_left()

        @pl.when(k == 1)
        def _():
            each(gd1, "finish")
            each(gd2, "far")
            each(gd2, "to_right")
            each(gd2, "to_left")

        @pl.when(k == 2)
        def _():
            near(2)
            xs.middle()

    weight_grad(pgt, ni, gu, gu1, ("far",), while_up)

    def settle(h):
        for ring in gu1:
            ring.settle(h)

    near(1)
    each(gu1, "add_first")
    give(gu1, 2, 1)
    near(3)
    give(gu1, 3)
    product(x)
    send_cross(3)
    each(gd2, "middle")
    settle(2)
    each(gu2, "far")
    near(0)
    give(gu1, 0)
    settle(1)
    each(gu2, "to_right")
    settle(3)
    each(gu2, "to_left")
    add_cross(3)
    each(gu2, "middle")
    settle(0)

    def store_rows(p, total):
        ig[pl.ds(p * half, half), :] = total.astype(BF16)

    xs.finish(store_rows)
    for i, ring in enumerate(gd2):

        def store_down(p, total, i=i):
            dg[wd_rows(2 * i + p), :] = total

        ring.finish(store_down)
    for i, ring in enumerate(gu2):

        def store_up(p, total, i=i):
            ug[:, wd_rows(2 * i + p)] = total.T

        ring.finish(store_up)
    for group in ("u", "o", "n", "D", "U", "x", "c"):
        w.drain(group)


def deliver(*refs):
    sem = refs[-1]
    copies = [pltpu.make_async_copy(refs[i], refs[3 + i], sem.at[i]) for i in range(3)]
    for copy in copies:
        copy.start()
    for copy in copies:
        copy.wait()


def local(normed_input, pre_act, out_grad, up_weight, down_weight):
    rows, d = out_grad.shape
    tokens, ff = pre_act.shape
    cols = down_weight.shape[1]
    quarter = ff // 4
    half = rows // 2
    grads = [
        pltpu.VMEM((2, 3, quarter, 4 * cols), BF16),
        pltpu.VMEM((2, 3, 4, quarter, cols), BF16),
        pltpu.VMEM((2, 3, quarter, cols), BF16),
        pltpu.VMEM((2, 3, quarter, cols), BF16),
    ]
    input_grad, up_grad, down_grad = pl.pallas_call(
        kernel,
        out_shape=(
            pltpu.VMEM((rows, d), BF16),
            pltpu.VMEM((cols, ff), F32),
            pltpu.VMEM((ff, cols), F32),
        ),
        in_specs=[pl.BlockSpec(memory_space=pltpu.HBM)] * 5,
        out_specs=(pl.BlockSpec(memory_space=pltpu.VMEM),) * 3,
        scratch_shapes=[
            pltpu.VMEM((tokens, d), BF16),
            pltpu.VMEM((tokens, d), BF16),
            pltpu.VMEM((4, ff, 4 * cols), BF16),
            pltpu.VMEM((4, 4, d // 16, ff), BF16),
            pltpu.VMEM((tokens, ff), BF16),
            pltpu.VMEM((ff, tokens), BF16),
            pltpu.VMEM((ff, tokens), BF16),
            pltpu.VMEM((8, rows, d), BF16),
            pltpu.VMEM((4, ff, 4 * cols), BF16),
            pltpu.VMEM((4, rows, d), BF16),
            pltpu.VMEM((2, 3, half, d), BF16),
            *grads,
            *grads,
            pltpu.SemaphoreType.DMA((SENDS,)),
            pltpu.SemaphoreType.DMA((RECVS,)),
            pltpu.SemaphoreType.DMA((5,)),
        ],
        compiler_params=pltpu.CompilerParams(
            collective_id=0,
            has_side_effects=True,
            vmem_limit_bytes=62800000,
        ),
        name="ffn_backward",
    )(normed_input, pre_act, out_grad, up_weight, down_weight)
    return pl.pallas_call(
        deliver,
        out_shape=(
            jax.ShapeDtypeStruct((rows, d), BF16),
            jax.ShapeDtypeStruct((cols, ff), F32),
            jax.ShapeDtypeStruct((ff, cols), F32),
        ),
        in_specs=[pl.BlockSpec(memory_space=pl.ANY)] * 3,
        out_specs=(pl.BlockSpec(memory_space=pl.ANY),) * 3,
        scratch_shapes=[pltpu.SemaphoreType.DMA((3,))],
        compiler_params=pltpu.CompilerParams(vmem_limit_bytes=4 * 2**20),
        name="deliver",
    )(input_grad, up_grad, down_grad)


def solution(mesh):
    placed = (
        P(("fs", "tp"), None),
        P("fs", "tp"),
        P(("fs", "tp"), None),
        P("fs", "tp"),
        P("tp", "fs"),
    )
    return jax.shard_map(
        local,
        mesh=mesh,
        in_specs=placed,
        out_specs=(P(("fs", "tp"), None), P("fs", "tp"), P("tp", "fs")),
        check_vma=False,
    )
```

```python
import math

import jax
import jax.numpy as jnp
from jax import lax
from jax.experimental import pallas as pl
from jax.experimental.pallas import tpu as pltpu
from jax.sharding import PartitionSpec as P

MESH = pl.DeviceIdType.MESH
F32 = jnp.float32
BF16 = jnp.bfloat16
SENDS, RECVS = 8, 37


def rem4(value):
    return lax.rem(value, 4)


def nt(a, b):
    return lax.dot_general(a, b, (((1,), (1,)), ((), ())), preferred_element_type=F32)


def nn(a, b):
    return jnp.dot(a, b, preferred_element_type=F32)


def size_of(ref):
    return 2 * math.prod(ref.shape)


class Wires:
    def __init__(self, send_sem, recv_sem, partner, filler):
        self.send_sem, self.recv_sem, self.partner = send_sem, recv_sem, partner
        self.filler = filler
        self.groups, self.keys, self.bytes = {}, {}, {}

    def group(self, name):
        return self.groups.setdefault(name, len(self.groups))

    def key(self, name):
        return self.keys.setdefault(name, len(self.keys))

    def copy(self, g, k, src, dst, device):
        return pltpu.make_async_remote_copy(
            src_ref=src,
            dst_ref=dst,
            send_sem=self.send_sem.at[g],
            recv_sem=self.recv_sem.at[k],
            device_id=device,
            device_id_type=MESH,
        )

    def send(self, group, key, src, dst, device):
        self.copy(self.group(group), self.key(key), src, dst, device).start()
        self.bytes[group] = self.bytes.get(group, 0) + size_of(src)

    def recv(self, key, size):
        ref = self.filler(size)
        self.copy(0, self.key(key), ref, ref, self.partner).wait_recv()

    def drain(self, group):
        ref = self.filler(self.bytes[group])
        self.copy(self.group(group), 0, ref, ref, self.partner).wait_send()


class Gather:
    share = 1

    def __init__(self, wires, group, tag, pos, right, left, piece):
        self.w, self.group, self.tag, self.pos = wires, group, tag, pos
        self.right, self.left, self.piece = right, left, piece
        self.size = size_of(piece(pos, 0))

    def wait(self, name, pieces):
        if self.share:
            self.w.recv((self.tag, name), self.share * pieces * self.size)

    def at(self, hop, p):
        return self.piece(rem4(self.pos + hop), p)

    def put(self, name, hop, p, device):
        ref = self.at(hop, p)
        self.w.send(self.group, (self.tag, name), ref, ref, device)

    def own(self):
        self.put("first", 0, 0, self.right)
        self.put("first", 0, 1, self.left)
        self.put("near", 0, 1, self.right)
        self.put("near", 0, 0, self.left)

    def forward(self):
        self.wait("first", 2)
        self.put("far", 3, 0, self.right)
        self.put("far", 1, 1, self.left)

    def near(self):
        self.wait("near", 2)

    def far(self):
        self.wait("far", 2)


class QuarterGather(Gather):
    def __init__(self, wires, group, tag, pos, right, left, piece, quarter):
        super().__init__(wires, group, tag, pos, right, left, piece)
        self.quarter = quarter

    def give(self, turn, *members):
        name = (self.tag, "near" if turn else "first")
        for h in members:
            for device, p in ((self.right, turn), (self.left, 1 - turn)):
                ref = self.quarter(self.pos, p, h)
                self.w.send(self.group, name, ref, ref, device)


class Scatter:
    share = 1

    def __init__(self, wires, group, tag, pos, right, left, piece, landing):
        self.w, self.group, self.tag, self.pos = wires, group, tag, pos
        self.right, self.left = right, left
        self.piece, self.landing = piece, landing
        self.size = size_of(piece(pos, 0))

    def wait(self, name, quarters):
        if self.share:
            self.w.recv((self.tag, name), self.share * quarters * self.size // 4)

    def at(self, hop, p):
        return self.piece(rem4(self.pos + hop), p)

    def put(self, name, side, m, hop, p):
        self.w.send(
            self.group,
            (self.tag, name),
            self.at(hop, p),
            self.landing(side, m),
            self.right if side == 0 else self.left,
        )

    def far(self):
        self.put("first", 0, 0, 2, 0)
        self.put("first", 1, 0, 2, 1)

    def to_right(self):
        self.put("last", 0, 1, 1, 1)

    def to_left(self):
        self.put("last", 1, 1, 3, 0)

    def add_first(self):
        self.wait("first", 8)
        for side, hop, p in ((0, 1, 0), (1, 3, 1)):
            came, mine = self.landing(side, 0), self.at(hop, p)
            mine[...] = (mine[...].astype(F32) + came[...].astype(F32)).astype(BF16)

    def middle(self):
        self.add_first()
        self.put("last", 0, 2, 1, 0)
        self.put("last", 1, 2, 3, 1)

    def finish(self, store=None):
        self.wait("last", 16)
        for p, near, far in ((1, 0, 1), (0, 1, 0)):
            first, second = self.landing(near, 1), self.landing(far, 2)
            mine = self.at(0, p)
            total = mine[...].astype(F32) + first[...].astype(F32) + second[...].astype(F32)
            if store is None:
                mine[...] = total.astype(BF16)
            else:
                store(p, total)


class QuarterScatter(Scatter):
    def __init__(self, wires, group, tag, pos, right, left, piece, landing, quarter, landed):
        super().__init__(wires, group, tag, pos, right, left, piece, landing)
        self.quarter, self.landed = quarter, landed

    def give(self, *members):
        for h in members:
            for side, hop, p in ((0, 1, 0), (1, 3, 1)):
                self.w.send(
                    self.group,
                    (self.tag, h),
                    self.quarter(rem4(self.pos + hop), p, h),
                    self.landed(side, 2, h),
                    self.right if side == 0 else self.left,
                )

    def near(self, *members):
        for h in members:
            for side, hop, p in ((0, 1, 1), (1, 3, 0)):
                self.w.send(
                    self.group,
                    (self.tag, h),
                    self.quarter(rem4(self.pos + hop), p, h),
                    self.landed(side, 1, h),
                    self.right if side == 0 else self.left,
                )

    def settle(self, h):
        self.wait(h, 4)
        for p, near, far in ((1, 0, 1), (0, 1, 0)):
            first, second = self.landed(near, 1, h), self.landed(far, 2, h)
            mine = self.quarter(self.pos, p, h)
            total = mine[...].astype(F32) + first[...].astype(F32) + second[...].astype(F32)
            mine[...] = total.astype(BF16)


def paired(first, second):
    second.tag, first.share, second.share = first.tag, 2, 0
    return first, second


def kernel(
    ni_hbm, pa_hbm, og_hbm, uw_hbm, dw_hbm,
    ig, ug, dg,
    ni, og, wd, wu, pg, ht, pgt, part, gd,
    cross, xland, zland_d, yland_d, yone_d, zone_d,
    zland_u, yland_u, yone_u, zone_u,
    send_sem, recv_sem, local_sem,
):
    fs, tp = lax.axis_index("fs"), lax.axis_index("tp")
    z, y, x, c = fs // 4, rem4(fs), tp // 2, lax.rem(tp, 2)
    x_right = {"fs": fs, "tp": rem4(x + 1) * 2 + c}
    x_left = {"fs": fs, "tp": rem4(x + 3) * 2 + c}
    y_right = {"fs": z * 4 + rem4(y + 1), "tp": tp}
    y_left = {"fs": z * 4 + rem4(y + 3), "tp": tp}
    z_right = {"fs": rem4(z + 1) * 4 + y, "tp": tp}
    z_left = {"fs": rem4(z + 3) * 4 + y, "tp": tp}
    partner = {"fs": fs, "tp": x * 2 + 1 - c}

    rows = og_hbm.shape[0]
    half = rows // 2
    ff, cols = dw_hbm.shape
    wide = 4 * cols
    quarter = ff // 4
    urows = uw_hbm.shape[0]
    tokens = pg.shape[0]

    line = 2 * og.shape[1]
    w = Wires(send_sem, recv_sem, partner, lambda size: og.at[pl.ds(0, size // line), :])

    def token_rows(ref, block):
        return ref.at[pl.ds(pl.multiple_of(block * rows, rows), rows), :]

    def lanes(i):
        return pl.ds(pl.multiple_of(i * cols, cols), cols)

    mine = [
        (dw_hbm, wd.at[z, :, lanes(y)]),
        (og_hbm, token_rows(og, tp)),
        (uw_hbm, wu.at[z, y]),
        (pa_hbm, pg),
        (ni_hbm, token_rows(ni, tp)),
    ]
    local = [
        pltpu.make_async_copy(src, dst, local_sem.at[i])
        for i, (src, dst) in enumerate(mine)
    ]
    barrier = pltpu.get_barrier_semaphore()
    for device in (x_right, x_left, y_right, y_left, z_right, z_left, partner):
        pl.semaphore_signal(barrier, inc=1, device_id=device, device_id_type=MESH)
    for i in (0, 2, 1, 3, 4):
        local[i].start()
    pl.semaphore_wait(barrier, 7)

    def wd_rows(p):
        return pl.ds(p * quarter, quarter)

    def wu_rows(p):
        return pl.ds(p * (urows // 4), urows // 4)

    def weight_rings(tag, one, z_group, y_group):
        return (
            (
                Gather(w, tag, tag + "a1", y, y_right, y_left, lambda i, p: one(z, i, p)),
                Gather(w, tag, tag + "b1", z, z_right, z_left, lambda i, p: one(i, y, 2 + p)),
            ),
            (
                Gather(w, tag, tag + "a2", z, z_right, z_left, lambda i, p: z_group(i, p)),
                Gather(w, tag, tag + "b2", y, y_right, y_left, lambda i, p: y_group(i, 2 + p)),
            ),
        )

    wd1, _ = weight_rings(
        "d",
        lambda zi, yi, p: wd.at[zi, wd_rows(p), lanes(yi)],
        lambda zi, p: wd.at[zi, wd_rows(p), :],
        lambda yi, p: wd.at[:, wd_rows(p), lanes(yi)],
    )
    wd2 = (
        QuarterGather(
            w, "d", "da2", z, z_right, z_left,
            lambda i, p: wd.at[i, wd_rows(p), :],
            lambda i, p, h: wd.at[i, wd_rows(p), lanes(rem4(y + h))],
        ),
        QuarterGather(
            w, "d", "db2", y, y_right, y_left,
            lambda i, p: wd.at[:, wd_rows(2 + p), lanes(i)],
            lambda i, p, h: wd.at[rem4(z + h), wd_rows(2 + p), lanes(i)],
        ),
    )
    wu1, wu2 = weight_rings(
        "u",
        lambda zi, yi, p: wu.at[zi, yi, wu_rows(p), :],
        lambda zi, p: wu.at[zi, :, wu_rows(p), :],
        lambda yi, p: wu.at[:, yi, wu_rows(p), :],
    )

    for pair in (wd1, wd2, wu1, wu2):
        paired(*pair)

    def token_piece(ref, core):
        def piece(i, p):
            start = pl.multiple_of((i * 2 + core) * rows + p * half, half)
            return ref.at[pl.ds(start, half), :]

        return piece

    rings = {
        "o": Gather(w, "o", "o", x, x_right, x_left, token_piece(og, c)),
        "n": Gather(w, "n", "n", x, x_right, x_left, token_piece(ni, c)),
    }

    def hand(tag, *pieces):
        for hop, p in pieces:
            ref = rings[tag].at(hop, p)
            w.send(tag, (tag, "cross"), ref, ref, partner)

    def handed(tag):
        w.recv((tag, "cross"), 8 * rings[tag].size)

    def token_own(tag):
        rings[tag].own()
        hand(tag, (0, 0), (0, 1))

    def token_forward(tag):
        rings[tag].forward()
        hand(tag, (3, 0), (1, 1))

    def token_near(tag):
        rings[tag].near()
        hand(tag, (3, 1), (1, 0))

    def token_far(tag):
        rings[tag].far()
        hand(tag, (2, 0), (2, 1))

    def each(pair, step):
        for ring in pair:
            getattr(ring, step)()

    def hidden(count, first):
        def body(j, carry):
            at = pl.multiple_of(j * 128, 128)
            active = jnp.maximum(pg[pl.ds(at, 128), :].astype(F32), 0.0)
            ht[:, pl.ds(at, 128)] = (active * active).astype(BF16).T
            return carry

        lax.fori_loop(first, first + count, body, 0)

    def give(pair, *what):
        for ring in pair:
            ring.give(*what)

    local[0].wait()
    each(wd1, "own")
    local[2].wait()
    each(wu1, "own")
    give(wd2, 0, 0)
    give(wd2, 1, 0)
    local[1].wait()
    token_own("o")
    local[3].wait()
    hidden(6, 0)
    each(wd1, "forward")
    each(wu1, "forward")
    hidden(6, 6)
    each(wd1, "near")
    give(wd2, 0, 1, 3)
    token_forward("o")
    each(wd1, "far")
    give(wd2, 0, 2)
    give(wd2, 1, 1, 3, 2)
    local[4].wait()
    token_own("n")
    each(wu1, "near")
    each(wu1, "far")
    each(wd2, "forward")
    each(wu2, "own")
    token_near("o")
    token_far("o")
    each(wd2, "near")
    each(wd2, "far")
    handed("o")

    block = 256

    def pre_grad(i, carry):
        at = pl.ds(pl.multiple_of(i * block, block), block)
        for n in range(2):
            units = pl.ds(n * ff // 2, ff // 2)
            weight = jnp.concatenate([wd[k, units, :] for k in range(4)], axis=1)
            grad = nt(og[at, :], weight)
            active = jnp.maximum(pg[at, units].astype(F32), 0.0)
            value = (2.0 * active * grad).astype(BF16)
            pg[at, units] = value
            pgt[units, at] = value.T

        @pl.when(i == 2)
        def _():
            each(wu2, "forward")

        @pl.when(i == 5)
        def _():
            token_forward("n")

        return carry

    lax.fori_loop(0, tokens // block, pre_grad, 0)

    def grad_rings(tag, grad, zland, yland, yone, zone):
        return (
            (
                Scatter(
                    w, tag, tag + "a1", z, z_right, z_left,
                    lambda i, p: grad.at[i, wd_rows(p), :],
                    lambda side, m: zland.at[side, m],
                ),
                Scatter(
                    w, tag, tag + "b1", y, y_right, y_left,
                    lambda i, p: grad.at[:, wd_rows(2 + p), lanes(i)],
                    lambda side, m: yland.at[side, m],
                ),
            ),
            (
                Scatter(
                    w, tag, tag + "a2", y, y_right, y_left,
                    lambda i, p: grad.at[z, wd_rows(p), lanes(i)],
                    lambda side, m: yone.at[side, m],
                ),
                Scatter(
                    w, tag, tag + "b2", z, z_right, z_left,
                    lambda i, p: grad.at[i, wd_rows(2 + p), lanes(y)],
                    lambda side, m: zone.at[side, m],
                ),
            ),
        )

    gd1, gd2 = grad_rings("D", gd, zland_d, yland_d, yone_d, zone_d)
    gu = wd
    _, gu2 = grad_rings("U", gu, zland_u, yland_u, yone_u, zone_u)
    gu1 = (
        QuarterScatter(
            w, "U", "Ua1", z, z_right, z_left,
            lambda i, p: gu.at[i, wd_rows(p), :],
            lambda side, m: zland_u.at[side, m],
            lambda i, p, h: gu.at[i, wd_rows(p), lanes(rem4(y + h))],
            lambda side, m, h: zland_u.at[side, m, :, lanes(rem4(y + h))],
        ),
        QuarterScatter(
            w, "U", "Ub1", y, y_right, y_left,
            lambda i, p: gu.at[:, wd_rows(2 + p), lanes(i)],
            lambda side, m: yland_u.at[side, m],
            lambda i, p, h: gu.at[rem4(z + h), wd_rows(2 + p), lanes(i)],
            lambda side, m, h: yland_u.at[side, m, rem4(z + h)],
        ),
    )
    for pair in (gd1, gd2, gu1, gu2):
        paired(*pair)
    upper = ff // 2

    def hop_of(k):
        return jnp.where(k == 0, 2, jnp.where(k == 1, 1, jnp.where(k == 2, 3, 0)))

    def weight_grad(left, right, grad, first, steps, extra):
        def body(k, carry):
            zi, yi = rem4(z + hop_of(k)), rem4(y + hop_of(k))
            strip = right[:, pl.ds(pl.multiple_of(zi * wide, wide), wide)]
            grad[zi, :upper, :] = nn(left[:upper, :], strip).astype(BF16)
            strip = jnp.concatenate(
                [right[:, pl.ds(pl.multiple_of(g * wide + yi * cols, cols), cols)] for g in range(4)],
                axis=1,
            )
            value = nn(left[upper:, :], strip).astype(BF16)
            for g in range(4):
                grad[g, upper:, lanes(yi)] = value[:, g * cols : (g + 1) * cols]

            if extra:
                extra(k)
            for turn, step in enumerate(steps):

                @pl.when(k == turn)
                def _(step=step):
                    each(first, step)

            return carry

        lax.fori_loop(0, 4, body, 0)

    weight_grad(ht, og, gd, gd1, ("far", "to_right", "to_left"), None)

    each(wu2, "near")
    each(wu2, "far")

    def share(block):
        return part.at[block]

    xs = Scatter(
        w, "x", "x", x, x_right, x_left,
        lambda i, p: part.at[i * 2 + c, pl.ds(p * half, half), :],
        lambda side, m: xland.at[side, m],
    )
    cross_base = [w.key(("c", k)) for k in range(4)][0]
    cross_group = w.group("c")
    w.bytes["c"] = size_of(cross)

    def product(xi):
        at = pl.ds(pl.multiple_of(xi * 2 * rows, 2 * rows), 2 * rows)
        for g in range(4):
            value = nt(pg[at, :], wu[g].reshape(4 * urows, ff)).astype(BF16)
            out = pl.ds(g * 4 * urows, 4 * urows)
            part[xi * 2, :, out] = value[:rows]
            part[xi * 2 + 1, :, out] = value[rows:]

    def send_cross(k):
        block = part.at[rem4(x + hop_of(k)) * 2 + 1 - c]
        w.copy(cross_group, cross_base + k, block, cross.at[k], partner).start()

    def add_cross(k):
        index = rem4(x + hop_of(k)) * 2 + c
        w.copy(cross_group, cross_base + k, cross.at[k], cross.at[k], partner).wait_recv()
        total = part[index].astype(F32) + cross[k].astype(F32)
        part[index] = total.astype(BF16)

    def input_grad(k, carry):
        xi = rem4(x + hop_of(k))
        product(xi)

        @pl.when(k == 2)
        def _():
            token_far("n")

        send_cross(k)

        @pl.when(k == 0)
        def _():
            token_near("n")

        @pl.when(k == 1)
        def _():
            each(gd1, "middle")
            add_cross(0)
            xs.far()

        @pl.when(k == 2)
        def _():
            add_cross(1)
            xs.to_right()

        return carry

    lax.fori_loop(0, 3, input_grad, 0)
    handed("n")
    w.drain("d")

    def near(*members):
        for ring in gu1:
            ring.near(*members)

    def while_up(k):
        @pl.when(k == 0)
        def _():
            add_cross(2)
            xs.to_left()

        @pl.when(k == 1)
        def _():
            each(gd1, "finish")
            each(gd2, "far")
            each(gd2, "to_right")
            each(gd2, "to_left")

        @pl.when(k == 2)
        def _():
            near(2)
            xs.middle()

    weight_grad(pgt, ni, gu, gu1, ("far",), while_up)

    def settle(h):
        for ring in gu1:
            ring.settle(h)

    near(1)
    each(gu1, "add_first")
    give(gu1, 2, 1)
    near(3)
    give(gu1, 3)
    product(x)
    send_cross(3)
    each(gd2, "middle")
    settle(2)
    each(gu2, "far")
    near(0)
    give(gu1, 0)
    settle(1)
    each(gu2, "to_right")
    settle(3)
    each(gu2, "to_left")
    add_cross(3)
    each(gu2, "middle")
    settle(0)

    def store_rows(p, total):
        ig[pl.ds(p * half, half), :] = total.astype(BF16)

    xs.finish(store_rows)
    for i, ring in enumerate(gd2):

        def store_down(p, total, i=i):
            dg[wd_rows(2 * i + p), :] = total

        ring.finish(store_down)
    for i, ring in enumerate(gu2):

        def store_up(p, total, i=i):
            ug[:, wd_rows(2 * i + p)] = total.T

        ring.finish(store_up)
    for group in ("u", "o", "n", "D", "U", "x", "c"):
        w.drain(group)


def deliver(*refs):
    sem = refs[-1]
    copies = [pltpu.make_async_copy(refs[i], refs[3 + i], sem.at[i]) for i in range(3)]
    for copy in copies:
        copy.start()
    for copy in copies:
        copy.wait()


def local(normed_input, pre_act, out_grad, up_weight, down_weight):
    rows, d = out_grad.shape
    tokens, ff = pre_act.shape
    cols = down_weight.shape[1]
    quarter = ff // 4
    half = rows // 2
    grads = [
        pltpu.VMEM((2, 3, quarter, 4 * cols), BF16),
        pltpu.VMEM((2, 3, 4, quarter, cols), BF16),
        pltpu.VMEM((2, 3, quarter, cols), BF16),
        pltpu.VMEM((2, 3, quarter, cols), BF16),
    ]
    input_grad, up_grad, down_grad = pl.pallas_call(
        kernel,
        out_shape=(
            pltpu.VMEM((rows, d), BF16),
            pltpu.VMEM((cols, ff), F32),
            pltpu.VMEM((ff, cols), F32),
        ),
        in_specs=[pl.BlockSpec(memory_space=pltpu.HBM)] * 5,
        out_specs=(pl.BlockSpec(memory_space=pltpu.VMEM),) * 3,
        scratch_shapes=[
            pltpu.VMEM((tokens, d), BF16),
            pltpu.VMEM((tokens, d), BF16),
            pltpu.VMEM((4, ff, 4 * cols), BF16),
            pltpu.VMEM((4, 4, d // 16, ff), BF16),
            pltpu.VMEM((tokens, ff), BF16),
            pltpu.VMEM((ff, tokens), BF16),
            pltpu.VMEM((ff, tokens), BF16),
            pltpu.VMEM((8, rows, d), BF16),
            pltpu.VMEM((4, ff, 4 * cols), BF16),
            pltpu.VMEM((4, rows, d), BF16),
            pltpu.VMEM((2, 3, half, d), BF16),
            *grads,
            *grads,
            pltpu.SemaphoreType.DMA((SENDS,)),
            pltpu.SemaphoreType.DMA((RECVS,)),
            pltpu.SemaphoreType.DMA((5,)),
        ],
        compiler_params=pltpu.CompilerParams(
            collective_id=0,
            has_side_effects=True,
            vmem_limit_bytes=62800000,
        ),
        name="ffn_backward",
    )(normed_input, pre_act, out_grad, up_weight, down_weight)
    return pl.pallas_call(
        deliver,
        out_shape=(
            jax.ShapeDtypeStruct((rows, d), BF16),
            jax.ShapeDtypeStruct((cols, ff), F32),
            jax.ShapeDtypeStruct((ff, cols), F32),
        ),
        in_specs=[pl.BlockSpec(memory_space=pl.ANY)] * 3,
        out_specs=(pl.BlockSpec(memory_space=pl.ANY),) * 3,
        scratch_shapes=[pltpu.SemaphoreType.DMA((3,))],
        compiler_params=pltpu.CompilerParams(vmem_limit_bytes=4 * 2**20),
        name="deliver",
    )(input_grad, up_grad, down_grad)


def solution(mesh):
    placed = (
        P(("fs", "tp"), None),
        P("fs", "tp"),
        P(("fs", "tp"), None),
        P("fs", "tp"),
        P("tp", "fs"),
    )
    return jax.shard_map(
        local,
        mesh=mesh,
        in_specs=placed,
        out_specs=(P(("fs", "tp"), None), P("fs", "tp"), P("tp", "fs")),
        check_vma=False,
    )
```
